128 devices in a mesh: fs: 16 (over z, y), tp: 8 (over x, core).
Axes of the slice: x: 4, y: 4, z: 4, core: 2. Of those that a mesh axis runs over, the one named last changes fastest.
Arguments:
- tokens: bfloat16 [16384, 2048], P(('fs', 'tp')), may hold values from -6 to 6
- norm_gain: float32 [2048], replicated, may hold values from 0.1 to 1.9
- up_weight: float32 [2048, 8192], P('fs', 'tp'), may hold values from -0.125 to 0.125
- down_weight: float32 [8192, 2048], P('tp', 'fs'), may hold values from -0.0625 to 0.0625
Outputs:
- mlp_out: bfloat16 [16384, 2048], P(('fs', 'tp'))
The draws below stay inside these ranges and needn't reach their ends.
All inputs are finite; a program needn't handle non-finite values.
Results may differ from the reference program's by a relative error of at most 0.0017.
Values may be sent and summed in bfloat16 or wider, within the bound.
A program may use at most 64 MiB of HBM per device.

```python
import jax
import jax.numpy as jnp
from jax import lax

D = 2048
FF = 8192
TOKENS = 16384


def levels(rng, shape, pieces, least, largest):
    level = 1.0
    for axis_at, shards_of in pieces:
        steps = jax.random.uniform(jax.random.fold_in(jax.random.fold_in(rng, 6), axis_at), (shards_of,), jnp.float32, least / len(pieces), largest / len(pieces))
        level = level * jnp.repeat(jnp.exp(steps), shape[axis_at] // shards_of).reshape((-1,) + (1,) * (len(shape) - 1 - axis_at))
    return level


def noise(rng, extent, width, bound, cuts=(), held_as=jnp.bfloat16):
    entries = jax.random.normal(rng, extent, jnp.float32) * width
    if len(cuts) > 0:
        entries = levels(rng, extent, cuts, -0.22, 0.18) * entries
    return jnp.clip(entries, min=-bound, max=bound).astype(held_as)


def setup_inputs(seed: int = 0) -> dict:
    streams_of = jax.random.split(jax.random.key(seed), 5)
    return {
        "tokens": noise(streams_of[0], (TOKENS, D), 1.0, 6.0, ((0, 128),)),
        "norm_gain": jnp.clip(1.0 + 0.18 * jax.random.normal(streams_of[1], (D,), jnp.float32), 0.1, 1.9),
        "up_weight": noise(streams_of[2], (D, FF), D ** -0.5, 0.125, ((0, 16), (1, 8)), jnp.float32),
        "down_weight": noise(streams_of[3], (FF, D), FF ** -0.5, 0.0625, ((0, 8), (1, 16)), jnp.float32),
    }


epsilon = 1e-06

def reference(tokens, norm_gain, up_weight, down_weight):
    up_low = up_weight.astype(jnp.bfloat16)
    down_low = down_weight.astype(jnp.bfloat16)
    block_rows = min(TOKENS, 1024)
    blocks = tokens.reshape(TOKENS // block_rows, block_rows, D)

    def one_block(rows):
        values = rows.astype(jnp.float32)
        scale = lax.rsqrt(lax.optimization_barrier(jnp.mean(values * values, axis=-1, keepdims=True)) + epsilon)
        normed = (values * scale * norm_gain).astype(jnp.bfloat16)
        pre = jnp.dot(normed, up_low, preferred_element_type=jnp.float32)
        hidden = jnp.square(jax.nn.relu(pre)).astype(jnp.bfloat16)
        return jnp.dot(hidden, down_low, preferred_element_type=jnp.float32).astype(jnp.bfloat16)
    return lax.map(one_block, blocks).reshape(TOKENS, D)
```

```python
import functools

import jax
import jax.numpy as jnp
from jax import lax
from jax.experimental import pallas as pl
from jax.experimental.pallas import tpu as pltpu
from jax.sharding import PartitionSpec as P

epsilon = 1e-06
MESH = pl.DeviceIdType.MESH
VMEM_LIMIT = 60_000_000
SIDE = 4
QUARTERS = 4
POWER = 9
PEAK = 11585.0
TINY = 1e-30


def encode(block):
    largest = jnp.max(jnp.abs(block), axis=0, keepdims=True)
    level = jnp.maximum(largest, TINY).astype(jnp.bfloat16)
    t = block * (PEAK / level.astype(jnp.float32))
    t2 = t * t
    t4 = t2 * t2
    return (t4 * t4 * t).astype(jnp.bfloat16), level


def decode(code, level):
    y = code.astype(jnp.float32)
    size = jnp.exp(jnp.log(jnp.maximum(jnp.abs(y), 1e-38)) * (1.0 / POWER)) * (level * (1.0 / PEAK))
    return jnp.where(y > 0.0, size, jnp.where(y < 0.0, -size, 0.0))


def kernel(
    tok_ref, gain_ref, up_ref, down_ref, out_ref,
    tok, up, down, acc, hidden, own, rs_out, rs_in,
    tok_send, tok_recv, up_recv, up_side, down_recv, down_side, sent, side_sent, rs_send, rs_recv,
):
    fs, tp = lax.axis_index("fs"), lax.axis_index("tp")
    z, y = fs // SIDE, lax.rem(fs, SIDE)
    x, c = tp // 2, lax.rem(tp, 2)
    other = 1 - c
    mine = fs
    rows = tok.shape[1]
    share = up.shape[3]
    piece = up.shape[4]
    width = down.shape[4]

    def ring(place, step):
        return lax.rem(place + (step + SIDE), SIDE)

    def at(dz, dy, dx):
        return (ring(z, dz) * SIDE + ring(y, dy), ring(x, dx) * 2 + c)

    sibling = (fs, x * 2 + other)

    def remote(src, dst, send, recv, to):
        return pltpu.make_async_remote_copy(
            src_ref=src, dst_ref=dst, send_sem=send, recv_sem=recv, device_id=to, device_id_type=MESH
        )

    barrier = pltpu.get_barrier_semaphore()
    peers = [at(1, 0, 0), at(-1, 0, 0), at(0, 1, 0), at(0, -1, 0), at(0, 0, 1), at(0, 0, -1), at(0, 0, 2), sibling]
    for to in peers:
        pl.semaphore_signal(barrier, inc=1, device_id=to, device_id_type=MESH)

    def block(h, ia, ib):
        dz, dy = (ia, ib) if h == 0 else (ib, ia)
        return ring(z, dz) * SIDE + ring(y, dy)

    class Gather:
        def __init__(self, number, buf, recv, side):
            self.number, self.buf, self.recv, self.side = number, buf, recv, side

        def send(self, h, ia, ib, j, axis, s):
            along_z = (axis == "a") == (h == 0)
            to = at(s, 0, 0) if along_z else at(0, s, 0)
            link = (0 if along_z else 2) + (0 if s > 0 else 1)
            ref = self.buf.at[c, block(h, ia, ib), 2 * h + j]
            remote(ref, ref, sent.at[self.number, link], self.recv.at[block(h, ia, ib), 2 * h + j], to).start()

        def wait(self, h, ia, ib, j):
            f = block(h, ia, ib)
            ref = self.buf.at[c, f, 2 * h + j]
            remote(ref, ref, sent.at[self.number, 0], self.recv.at[f, 2 * h + j], sibling).wait_recv()

        def over(self, h, ia, ib):
            f = block(h, ia, ib)
            ref = self.buf.at[c, f, pl.ds(2 * h, 2)]
            remote(ref, ref, side_sent.at[self.number], self.side.at[f, h], sibling).start()

        def wait_over(self, h, ia, ib):
            f = block(h, ia, ib)
            ref = self.buf.at[other, f, pl.ds(2 * h, 2)]
            remote(ref, ref, side_sent.at[self.number], self.side.at[f, h], sibling).wait_recv()

        def first(self):
            for turn in (0, 1):
                for h in (0, 1):
                    for s in (1, -1):
                        self.send(h, 0, 0, turn if s > 0 else 1 - turn, "a", s)
            for turn in (0, 1):
                for h in (0, 1):
                    for s in (1, -1):
                        self.send(h, 0, 0, turn if s > 0 else 1 - turn, "b", s)
            for h in (0, 1):
                self.over(h, 0, 0)

        def near(self):
            for turn in (0, 1):
                for h in (0, 1):
                    for s in (1, -1):
                        j = turn if s > 0 else 1 - turn
                        self.wait(h, -s, 0, j)
                        if turn == 0:
                            self.send(h, -s, 0, j, "a", s)
                        for side in (1, -1):
                            self.send(h, -s, 0, j, "b", side)
            for h in (0, 1):
                for s in (1, -1):
                    self.over(h, -s, 0)

        def cross(self, ia):
            for turn in (0, 1):
                for h in (0, 1):
                    for s in (1, -1):
                        j = turn if s > 0 else 1 - turn
                        self.wait(h, ia, -s, j)
                        if turn == 0:
                            self.send(h, ia, -s, j, "b", s)
            for h in (0, 1):
                for s in (1, -1):
                    self.over(h, ia, -s)

        def far(self):
            for h in (0, 1):
                for j in (0, 1):
                    self.wait(h, 2, 0, j)
                    for side in (1, -1):
                        self.send(h, 2, 0, j, "b", side)
            for h in (0, 1):
                self.over(h, 2, 0)

        def last(self, ia):
            for h in (0, 1):
                for j in (0, 1):
                    self.wait(h, ia, 2, j)
                self.over(h, ia, 2)

        def drain(self):
            count = self.buf.shape[1] - 1
            ref = self.buf.at[0, pl.ds(0, count), 0]
            for link in range(4):
                remote(ref, ref, sent.at[self.number, link], sent.at[self.number, link], sibling).wait_send()
            whole = self.buf.at[0]
            remote(whole, whole, side_sent.at[self.number], side_sent.at[self.number], sibling).wait_send()

    ups = Gather(0, up, up_recv, up_side)
    downs = Gather(1, down, down_recv, down_side)

    for q in range(QUARTERS):
        up[c, mine, q] = up_ref[:, q * piece:(q + 1) * piece].astype(jnp.bfloat16)
    pl.semaphore_wait(barrier, len(peers))
    ups.first()

    values = tok_ref[...].astype(jnp.float32)
    scale = lax.rsqrt(jnp.mean(values * values, axis=-1, keepdims=True) + epsilon)
    tok[x] = (values * scale * gain_ref[...]).astype(jnp.bfloat16)
    half = rows // 2

    def token_copy(slot, part, s, number):
        ref = tok.at[slot, pl.ds(part * half, half)]
        return remote(ref, ref, tok_send.at[number], tok_recv.at[slot, part], at(0, 0, s))

    own_copies = []
    for turn in (0, 1):
        for s in (1, -1):
            part = turn if s > 0 else 1 - turn
            own_copies.append(token_copy(x, part, s, len(own_copies)))
            own_copies[-1].start()
    for q in range(QUARTERS):
        down[c, mine, q] = down_ref[q * share * 2:(q + 1) * share * 2, :].astype(jnp.bfloat16)

    def token_wait(slot, part):
        token_copy(slot, part, 1, 0).wait_recv()

    ups.near()
    for s in (1, -1):
        part = 0 if s > 0 else 1
        slot = ring(x, -s)
        token_wait(slot, part)
        own_copies.append(token_copy(slot, part, s, len(own_copies)))
        own_copies[-1].start()
    ups.cross(0)
    ups.far()
    ups.cross(-1)
    ups.cross(1)
    ups.last(0)
    ups.cross(2)
    downs.first()

    for s in (1, -1):
        token_wait(ring(x, -s), 1 if s > 0 else 0)
    for part in (0, 1):
        token_wait(ring(x, 2), part)

    tokens = tok.shape[0] * rows

    def expand(h, places, begin, end):
        for place in places:
            ups.wait_over(h, *place)
        numbers = [block(h, *place) for place in places]

        def columns(n, carry):
            core, q = n // 2, 2 * h + lax.rem(n, 2)
            slot = core * QUARTERS + q
            left = jnp.concatenate(
                [tok[:, :, pl.ds(pl.multiple_of(f * share, share), share)].reshape(tokens, share) for f in numbers], axis=1
            )
            right = jnp.concatenate([up[core, f, q] for f in numbers], axis=0)
            pre = jnp.dot(left, right, preferred_element_type=jnp.float32)
            if not begin:
                pre = pre + acc[slot]
            if end:
                hidden[slot] = jnp.square(jnp.maximum(pre, 0.0)).astype(jnp.bfloat16)
            else:
                acc[slot] = pre
            return carry

        lax.fori_loop(0, 4, columns, 0)

    for h in (0, 1):
        expand(h, [(0, 0), (-1, 0), (1, 0), (2, 0)], True, False)
    for h in (0, 1):
        expand(h, [(0, -1), (0, 1), (-1, -1), (-1, 1)], False, False)
    for h in (0, 1):
        expand(h, [(1, -1), (1, 1), (2, -1), (2, 1)], False, False)
    for ia in (-1, 1, 2):
        ups.last(ia)
    for h in (0, 1):
        expand(h, [(0, 2), (-1, 2), (1, 2), (2, 2)], False, True)

    def spot(dz, dy):
        return ring(z, dz) * SIDE + ring(y, dy)

    hops = (1, -1, 2)

    def rs_copy(pair, number):
        return remote(
            rs_out.at[pair, number], rs_in.at[pair, number], rs_send.at[pair, number], rs_recv.at[pair, number],
            at(0, 0, hops[number]),
        )

    def project(pair, places):
        for dz, dy in places:
            downs.wait_over(0, dz, dy)
            downs.wait_over(1, dy, dz)
        numbers = [spot(*place) for place in places]
        total = None
        for core in range(2):
            for q in range(QUARTERS):
                right = jnp.concatenate([down[core, f, q] for f in numbers], axis=1)
                part = jnp.dot(hidden[core * QUARTERS + q], right, preferred_element_type=jnp.float32)
                total = part if total is None else total + part
        terms = acc.at[pair]
        terms[...] = total
        for number, hop in enumerate(hops):
            to = ring(x, hop)
            code, level = encode(terms[pl.ds(pl.multiple_of(to * rows, rows), rows), :])
            rs_out[pair, number, 0:rows] = code
            rs_out[pair, number, rows:rows + 16] = jnp.broadcast_to(level, (16, level.shape[1]))
            rs_copy(pair, number).start()
        own[pair] = terms[pl.ds(pl.multiple_of(x * rows, rows), rows), :]

    def finish(pair, places):
        total = own[pair]
        for number in range(len(hops)):
            rs_copy(pair, number).wait_recv()
            level = rs_in[pair, number, rows:rows + 16].astype(jnp.float32)[0:1]
            total = total + decode(rs_in[pair, number, 0:rows], level)
        low = total.astype(jnp.bfloat16)
        for n, place in enumerate(places):
            out_ref[:, pl.ds(pl.multiple_of(spot(*place) * width, width), width)] = low[:, n * width:(n + 1) * width]

    pairs = [
        [(0, 0), (-1, 0)], [(1, 0), (0, -1)], [(0, 1), (2, 0)], [(0, 2), (-1, -1)],
        [(-1, 1), (1, -1)], [(1, 1), (2, 1)], [(2, -1), (1, 2)], [(-1, 2), (2, 2)],
    ]
    downs.near()
    downs.cross(0)
    project(0, pairs[0])
    downs.far()
    project(1, pairs[1])
    downs.cross(-1)
    downs.cross(1)
    downs.last(0)
    project(2, pairs[2])
    project(3, pairs[3])
    downs.cross(2)
    project(4, pairs[4])
    finish(0, pairs[0])
    finish(1, pairs[1])
    for ia in (-1, 1, 2):
        downs.last(ia)
    project(5, pairs[5])
    project(6, pairs[6])
    project(7, pairs[7])
    for pair in range(2, 8):
        finish(pair, pairs[pair])

    for copy in own_copies:
        copy.wait_send()
    for pair in range(8):
        for number in range(len(hops)):
            rs_copy(pair, number).wait_send()
    ups.drain()
    downs.drain()


def solution(mesh):
    fs, tp = mesh.shape["fs"], mesh.shape["tp"]
    placed = (P(("fs", "tp"), None), P(), P("fs", "tp"), P("tp", "fs"))

    def whole(tokens, norm_gain, up_weight, down_weight):
        rows, depth = tokens.shape
        share, span = up_weight.shape
        width = down_weight.shape[1]
        piece = span // QUARTERS
        groups = tp // 2
        vm, dma = pltpu.VMEM, pltpu.SemaphoreType.DMA
        low, full = jnp.bfloat16, jnp.float32
        at_vmem = pl.BlockSpec(memory_space=pltpu.VMEM)
        pairs = fs // 2
        return pl.pallas_call(
            kernel,
            out_shape=jax.ShapeDtypeStruct((rows, depth), low),
            in_specs=[at_vmem] * 4,
            out_specs=at_vmem,
            scratch_shapes=[
                vm((groups, rows, depth), low),
                vm((2, fs, QUARTERS, share, piece), low),
                vm((2, fs, QUARTERS, piece, width), low),
                vm((2 * QUARTERS, groups * rows, piece), full),
                vm((2 * QUARTERS, groups * rows, piece), low),
                vm((pairs, rows, 2 * width), full),
                vm((pairs, 3, rows + 16, 2 * width), low),
                vm((pairs, 3, rows + 16, 2 * width), low),
                dma((6,)), dma((groups, 2)),
                dma((fs, QUARTERS)), dma((fs, 2)), dma((fs, QUARTERS)), dma((fs, 2)),
                dma((2, 4)), dma((2,)), dma((pairs, 3)), dma((pairs, 3)),
            ],
            compiler_params=pltpu.CompilerParams(
                collective_id=0, has_side_effects=True, vmem_limit_bytes=VMEM_LIMIT
            ),
        )(tokens, norm_gain.reshape(1, depth), up_weight, down_weight)

    return jax.shard_map(
        whole, mesh=mesh, in_specs=placed, out_specs=P(("fs", "tp"), None), check_vma=False
    )
```

```python
import functools

import jax
import jax.numpy as jnp
from jax import lax
from jax.experimental import pallas as pl
from jax.experimental.pallas import tpu as pltpu
from jax.sharding import PartitionSpec as P

epsilon = 1e-06
MESH = pl.DeviceIdType.MESH
VMEM_LIMIT = 60_000_000
SIDE = 4
QUARTERS = 4
LANES = 128
POWER = 9
PEAK = 11585.0
TINY = 1e-30


def encode(block):
    largest = jnp.max(jnp.abs(block), axis=0, keepdims=True)
    level = largest[:, :LANES]
    for start in range(LANES, block.shape[1], LANES):
        level = jnp.maximum(level, largest[:, start:start + LANES])
    level = jnp.maximum(level, TINY).astype(jnp.bfloat16)
    factor = PEAK / level.astype(jnp.float32)
    codes = []
    for start in range(0, block.shape[1], LANES):
        t = block[:, start:start + LANES] * factor
        t2 = t * t
        t4 = t2 * t2
        codes.append((t4 * t4 * t).astype(jnp.bfloat16))
    return codes, jnp.broadcast_to(level, (16, LANES))


def decode(code, level):
    y = code.astype(jnp.float32)
    size = jnp.exp(jnp.log(jnp.maximum(jnp.abs(y), 1e-38)) * (1.0 / POWER)) * (level * (1.0 / PEAK))
    return jnp.where(y > 0.0, size, jnp.where(y < 0.0, -size, 0.0))


def kernel(
    tok_hbm, gain_hbm, up_hbm, down_hbm, out_ref,
    tok_ref, gain_ref, up_ref, down_ref, tok, up, down, acc, hidden, one_out, one_in, two_out, two_in,
    load, tok_send, tok_recv, arrived, crossed, sent, side_sent, one_send, one_recv, two_send, two_recv,
):
    fs, tp = lax.axis_index("fs"), lax.axis_index("tp")
    z, y = fs // SIDE, lax.rem(fs, SIDE)
    x, c = tp // 2, lax.rem(tp, 2)
    other = 1 - c
    mine = fs
    rows = tok.shape[1]
    share = up.shape[3]
    piece = up.shape[4]
    width = down.shape[4]

    def ring(place, step):
        return lax.rem(place + (step + SIDE), SIDE)

    def at(dz, dy, dx):
        return (ring(z, dz) * SIDE + ring(y, dy), ring(x, dx) * 2 + c)

    sibling = (fs, x * 2 + other)

    def remote(src, dst, send, recv, to):
        return pltpu.make_async_remote_copy(
            src_ref=src, dst_ref=dst, send_sem=send, recv_sem=recv, device_id=to, device_id_type=MESH
        )

    barrier = pltpu.get_barrier_semaphore()
    peers = [at(1, 0, 0), at(-1, 0, 0), at(0, 1, 0), at(0, -1, 0), at(0, 0, 1), at(0, 0, -1), sibling]
    for to in peers:
        pl.semaphore_signal(barrier, inc=1, device_id=to, device_id_type=MESH)

    loads = [
        pltpu.make_async_copy(src, dst, load.at[n])
        for n, (src, dst) in enumerate([(up_hbm, up_ref), (tok_hbm, tok_ref), (gain_hbm, gain_ref), (down_hbm, down_ref)])
    ]
    for copy in loads:
        copy.start()

    def block(h, ia, ib):
        dz, dy = (ia, ib) if h == 0 else (ib, ia)
        return ring(z, dz) * SIDE + ring(y, dy)

    NEAR, CROSS, FAR, LAST = 0, 2, 10, 11
    spot_of = {0: 0, -1: 1, 1: 2, 2: 3}

    class Gather:
        def __init__(self, number, buf):
            self.number, self.buf = number, buf

        def send(self, h, ia, ib, j, axis, s, group):
            along_z = (axis == "a") == (h == 0)
            to = at(s, 0, 0) if along_z else at(0, s, 0)
            ref = self.buf.at[c, block(h, ia, ib), 2 * h + j]
            remote(ref, ref, sent.at[self.number], arrived.at[self.number, group], to).start()

        def wait(self, group):
            ref = self.buf.at[c, pl.ds(0, 4), 0]
            remote(ref, ref, sent.at[self.number], arrived.at[self.number, group], sibling).wait_recv()

        def over(self, places, event):
            for h in (0, 1):
                for ia, ib in places:
                    ref = self.buf.at[c, block(h, ia, ib), pl.ds(2 * h, 2)]
                    remote(ref, ref, side_sent.at[self.number], crossed.at[self.number, event], sibling).start()

        def wait_over(self, event):
            count = 2 if event in (0, 2, 7, 8, 9, 10) else 4
            ref = self.buf.at[other, pl.ds(0, count), pl.ds(0, 2)]
            remote(ref, ref, side_sent.at[self.number], crossed.at[self.number, event], sibling).wait_recv()

        def first(self):
            for axis in ("a", "b"):
                for turn in (0, 1):
                    for h in (0, 1):
                        for s in (1, -1):
                            j = turn if s > 0 else 1 - turn
                            self.send(h, 0, 0, j, axis, s, (NEAR if axis == "a" else CROSS) + turn)
            self.over([(0, 0)], 0)

        def out(self, h, ia, j):
            for s in (1, -1):
                turn = j if s > 0 else 1 - j
                self.send(h, ia, 0, j, "b", s, CROSS + 2 * spot_of[ia] + turn)

        def near(self):
            for turn in (0, 1):
                self.wait(NEAR + turn)
                if turn == 0:
                    for h in (0, 1):
                        for s in (1, -1):
                            self.send(h, -s, 0, 0 if s > 0 else 1, "a", s, FAR)
                for h in (0, 1):
                    for s in (1, -1):
                        self.out(h, -s, turn if s > 0 else 1 - turn)
            self.over([(-1, 0), (1, 0)], 1)

        def cross(self, ia):
            for turn in (0, 1):
                self.wait(CROSS + 2 * spot_of[ia] + turn)
                if turn == 0:
                    for h in (0, 1):
                        for s in (1, -1):
                            self.send(h, ia, -s, 0 if s > 0 else 1, "b", s, LAST + spot_of[ia])
            self.over([(ia, -1), (ia, 1)], 3 + spot_of[ia])

        def far(self):
            self.wait(FAR)
            for j in (0, 1):
                for h in (0, 1):
                    self.out(h, 2, j)
            self.over([(2, 0)], 2)

        def last(self, ia):
            self.wait(LAST + spot_of[ia])
            self.over([(ia, 2)], 7 + spot_of[ia])

        def drain(self):
            ref = self.buf.at[0, pl.ds(0, self.buf.shape[1] - 1)]
            remote(ref, ref, sent.at[self.number], sent.at[self.number], sibling).wait_send()
            whole = self.buf.at[0]
            remote(whole, whole, side_sent.at[self.number], side_sent.at[self.number], sibling).wait_send()

    ups = Gather(0, up)
    downs = Gather(1, down)

    loads[0].wait()
    for q in range(QUARTERS):
        up[c, mine, q] = up_ref[:, q * piece:(q + 1) * piece].astype(jnp.bfloat16)
    pl.semaphore_wait(barrier, len(peers))
    ups.first()

    loads[1].wait()
    loads[2].wait()
    values = tok_ref[...].astype(jnp.float32)
    scale = lax.rsqrt(jnp.mean(values * values, axis=-1, keepdims=True) + epsilon)
    tok[x] = (values * scale * gain_ref[...]).astype(jnp.bfloat16)
    half = rows // 2

    def token_send(slot, part, s, group):
        ref = tok.at[slot, pl.ds(part * half, half)]
        remote(ref, ref, tok_send, tok_recv.at[group], at(0, 0, s)).start()

    def token_wait(group):
        ref = tok.at[0]
        remote(ref, ref, tok_send, tok_recv.at[group], sibling).wait_recv()

    for turn in (0, 1):
        for s in (1, -1):
            token_send(x, turn if s > 0 else 1 - turn, s, turn)
    loads[3].wait()
    for q in range(QUARTERS):
        down[c, mine, q] = down_ref[q * piece:(q + 1) * piece, :].astype(jnp.bfloat16)

    relative = (0, 1, -1, 2)

    def expand(places, begin, end, first_row, last_row):
        for h in (0, 1):
            numbers = [block(h, *place) for place in places]
            left = jnp.concatenate([
                jnp.concatenate(
                    [tok[ring(x, relative[r]), :, pl.ds(pl.multiple_of(f * share, share), share)] for f in numbers], axis=1
                ) for r in range(first_row, last_row)
            ], axis=0)
            span = slice(first_row * rows, last_row * rows)
            for core in (0, 1):
                slots = [core * QUARTERS + 2 * h + j for j in (0, 1)]
                right = jnp.concatenate([
                    jnp.concatenate([up[core, f, 2 * h + j] for f in numbers], axis=0) for j in (0, 1)
                ], axis=1)
                pre = jnp.dot(left, right, preferred_element_type=jnp.float32)
                for j, slot in enumerate(slots):
                    new = pre[:, j * piece:(j + 1) * piece]
                    if not begin:
                        new = new + acc[slot, span]
                    if end:
                        hidden[slot, span] = jnp.square(jnp.maximum(new, 0.0)).astype(jnp.bfloat16)
                    else:
                        acc[slot, span] = new

    groups = [
        [(0, 0), (-1, 0), (1, 0), (2, 0)], [(0, -1), (0, 1), (-1, -1), (-1, 1)],
        [(1, -1), (1, 1), (2, -1), (2, 1)], [(0, 2), (-1, 2), (1, 2), (2, 2)],
    ]

    ups.near()
    ups.cross(0)
    ups.far()
    token_wait(0)
    for s in (1, -1):
        token_send(ring(x, -s), 0 if s > 0 else 1, s, 2)
    ups.cross(-1)
    ups.cross(1)
    token_wait(1)
    for event in (0, 1, 2):
        ups.wait_over(event)
    expand(groups[0], True, False, 0, 3)
    ups.last(0)
    for event in (3, 4):
        ups.wait_over(event)
    expand(groups[1], False, False, 0, 3)
    ups.cross(2)
    downs.first()
    token_wait(2)
    expand(groups[0], True, False, 3, 4)
    expand(groups[1], False, False, 3, 4)
    ups.last(-1)
    for event in (5, 6):
        ups.wait_over(event)
    expand(groups[2], False, False, 0, 4)
    ups.last(1)
    ups.last(2)
    for event in (7, 8, 9, 10):
        ups.wait_over(event)
    expand(groups[3], False, True, 0, 4)

    def spot(dz, dy):
        return ring(z, dz) * SIDE + ring(y, dy)

    def one_copy(pair, way):
        return remote(
            one_out.at[pair, way], one_in.at[pair, way], one_send, one_recv.at[pair], at(0, 0, 1 - 2 * way)
        )

    def two_copy(pair, way):
        return remote(
            two_out.at[pair, way], two_in.at[pair, way], two_send, two_recv.at[pair], at(0, 0, 1 - 2 * way)
        )

    def project(pair):
        numbers = [spot(*place) for place in pairs[pair]]
        left = jnp.concatenate([hidden[slot] for slot in range(2 * QUARTERS)], axis=1)
        right = jnp.concatenate([
            jnp.concatenate([down[core, f, q] for f in numbers], axis=1) for core in (0, 1) for q in range(QUARTERS)
        ], axis=0)
        acc[pair] = jnp.dot(left, right, preferred_element_type=jnp.float32)
        for way in (0, 1):
            (code,), level = encode(acc[pair, 3 * rows:, way * width:(way + 1) * width])
            one_out[pair, way, 0:rows] = code
            one_out[pair, way, rows:rows + 16] = level
            one_copy(pair, way).start()

    def relay(pair):
        ref = one_in.at[pair]
        remote(ref, ref, one_send, one_recv.at[pair], sibling).wait_recv()
        for way in (0, 1):
            level = one_in[pair, way, rows:rows + 16].astype(jnp.float32)[0:1]
            taken = decode(one_in[pair, way, 0:rows], level)
            halves = [acc[pair, (1 + way) * rows:(2 + way) * rows, n * width:(n + 1) * width] for n in (0, 1)]
            halves[way] = halves[way] + taken
            codes, level = encode(jnp.concatenate(halves, axis=1))
            for n in (0, 1):
                two_out[pair, way, n * rows:(n + 1) * rows] = codes[n]
            two_out[pair, way, 2 * rows:2 * rows + 16] = level
            two_copy(pair, way).start()

    def finish(pair):
        ref = two_in.at[pair]
        remote(ref, ref, two_send, two_recv.at[pair], sibling).wait_recv()
        levels = [two_in[pair, way, 2 * rows:2 * rows + 16].astype(jnp.float32)[0:1] for way in (0, 1)]
        for n, place in enumerate(pairs[pair]):
            total = acc[pair, 0:rows, n * width:(n + 1) * width]
            for way in (0, 1):
                total = total + decode(two_in[pair, way, n * rows:(n + 1) * rows], levels[way])
            out_ref[:, pl.ds(pl.multiple_of(spot(*place) * width, width), width)] = total.astype(jnp.bfloat16)

    pairs = [
        [(0, 0), (-1, 0)], [(1, 0), (0, -1)], [(0, 1), (2, 0)], [(0, 2), (-1, -1)],
        [(-1, 1), (1, -1)], [(1, 1), (2, 1)], [(2, -1), (1, 2)], [(-1, 2), (2, 2)],
    ]
    downs.near()
    downs.cross(0)
    for event in (0, 1, 3):
        downs.wait_over(event)
    project(0)
    downs.far()
    project(1)
    downs.cross(-1)
    relay(0)
    downs.cross(1)
    downs.last(0)
    relay(1)
    for event in (2, 4, 5, 7):
        downs.wait_over(event)
    project(2)
    downs.cross(2)
    project(3)
    relay(2)
    project(4)
    relay(3)
    finish(0)
    finish(1)
    relay(4)
    finish(2)
    for ia in (-1, 1, 2):
        downs.last(ia)
    for event in (6, 8, 9, 10):
        downs.wait_over(event)
    project(5)
    project(6)
    relay(5)
    project(7)
    relay(6)
    finish(3)
    relay(7)
    finish(4)
    finish(5)
    finish(6)
    finish(7)

    ref = tok.at[pl.ds(0, 3)]
    remote(ref, ref, tok_send, tok_send, sibling).wait_send()
    remote(one_out, one_out, one_send, one_send, sibling).wait_send()
    remote(two_out, two_out, two_send, two_send, sibling).wait_send()
    ups.drain()
    downs.drain()


def solution(mesh):
    fs, tp = mesh.shape["fs"], mesh.shape["tp"]
    placed = (P(("fs", "tp"), None), P(), P("fs", "tp"), P("tp", "fs"))

    def whole(tokens, norm_gain, up_weight, down_weight):
        rows, depth = tokens.shape
        share, span = up_weight.shape
        width = down_weight.shape[1]
        piece = span // QUARTERS
        groups = tp // 2
        vm, dma = pltpu.VMEM, pltpu.SemaphoreType.DMA
        low, full = jnp.bfloat16, jnp.float32
        pairs = fs // 2
        return pl.pallas_call(
            kernel,
            out_shape=jax.ShapeDtypeStruct((rows, depth), low),
            in_specs=[pl.BlockSpec(memory_space=pltpu.HBM)] * 4,
            out_specs=pl.BlockSpec(memory_space=pltpu.VMEM),
            scratch_shapes=[
                vm((rows, depth), low),
                vm((1, depth), full),
                vm((share, span), full),
                vm((span, width), full),
                vm((groups, rows, depth), low),
                vm((2, fs, QUARTERS, share, piece), low),
                vm((2, fs, QUARTERS, piece, width), low),
                vm((2 * QUARTERS, groups * rows, piece), full),
                vm((2 * QUARTERS, groups * rows, piece), low),
                vm((pairs, 2, rows + 16, LANES), low),
                vm((pairs, 2, rows + 16, LANES), low),
                vm((pairs, 2, 2 * rows + 16, LANES), low),
                vm((pairs, 2, 2 * rows + 16, LANES), low),
                dma((4,)), dma, dma((3,)),
                dma((2, 15)), dma((2, 11)), dma((2,)), dma((2,)), dma, dma((pairs,)), dma, dma((pairs,)),
            ],
            compiler_params=pltpu.CompilerParams(
                collective_id=0, has_side_effects=True, vmem_limit_bytes=VMEM_LIMIT
            ),
        )(tokens, norm_gain.reshape(1, depth), up_weight, down_weight)

    return jax.shard_map(
        whole, mesh=mesh, in_specs=placed, out_specs=P(("fs", "tp"), None), check_vma=False
    )
```

```python
import functools

import jax
import jax.numpy as jnp
from jax import lax
from jax.experimental import pallas as pl
from jax.experimental.pallas import tpu as pltpu
from jax.sharding import PartitionSpec as P

epsilon = 1e-06
MESH = pl.DeviceIdType.MESH
VMEM_LIMIT = 60_000_000
SIDE = 4
QUARTERS = 4
LANES = 128
POWER = 9
PEAK = 11585.0
TINY = 1e-30


def encode(block):
    largest = jnp.max(jnp.abs(block), axis=0, keepdims=True)
    level = largest[:, :LANES]
    for start in range(LANES, block.shape[1], LANES):
        level = jnp.maximum(level, largest[:, start:start + LANES])
    level = jnp.maximum(level, TINY).astype(jnp.bfloat16)
    factor = PEAK / level.astype(jnp.float32)
    codes = []
    for start in range(0, block.shape[1], LANES):
        t = block[:, start:start + LANES] * factor
        t2 = t * t
        t4 = t2 * t2
        codes.append((t4 * t4 * t).astype(jnp.bfloat16))
    return codes, jnp.broadcast_to(level, (16, LANES))


def decode(code, level):
    y = code.astype(jnp.float32)
    size = jnp.exp(jnp.log(jnp.maximum(jnp.abs(y), 1e-38)) * (1.0 / POWER)) * (level * (1.0 / PEAK))
    return jnp.where(y > 0.0, size, jnp.where(y < 0.0, -size, 0.0))


def kernel(
    tok_hbm, gain_hbm, up_hbm, down_hbm, out_ref,
    tok_ref, gain_ref, up_ref, down_ref, tok, up, down, acc, hidden, one_out, one_in, two_out, two_in,
    load, tok_send, tok_recv, arrived, crossed, sent, side_sent, one_send, one_recv, two_send, two_recv,
):
    fs, tp = lax.axis_index("fs"), lax.axis_index("tp")
    z, y = fs // SIDE, lax.rem(fs, SIDE)
    x, c = tp // 2, lax.rem(tp, 2)
    other = 1 - c
    mine = fs
    rows = tok.shape[1]
    share = up.shape[3]
    piece = up.shape[4]
    width = down.shape[4]

    def ring(place, step):
        return lax.rem(place + (step + SIDE), SIDE)

    def at(dz, dy, dx):
        return (ring(z, dz) * SIDE + ring(y, dy), ring(x, dx) * 2 + c)

    sibling = (fs, x * 2 + other)

    def remote(src, dst, send, recv, to):
        return pltpu.make_async_remote_copy(
            src_ref=src, dst_ref=dst, send_sem=send, recv_sem=recv, device_id=to, device_id_type=MESH
        )

    barrier = pltpu.get_barrier_semaphore()
    peers = [at(1, 0, 0), at(-1, 0, 0), at(0, 1, 0), at(0, -1, 0), at(0, 0, 1), at(0, 0, -1), sibling]
    for to in peers:
        pl.semaphore_signal(barrier, inc=1, device_id=to, device_id_type=MESH)

    loads = [
        pltpu.make_async_copy(src, dst, load.at[n])
        for n, (src, dst) in enumerate([(up_hbm, up_ref), (tok_hbm, tok_ref), (gain_hbm, gain_ref), (down_hbm, down_ref)])
    ]
    for copy in loads:
        copy.start()

    def block(h, ia, ib):
        dz, dy = (ia, ib) if h == 0 else (ib, ia)
        return ring(z, dz) * SIDE + ring(y, dy)

    ways = (1, -1)
    NEAR, OWN, FAR, BACK, WIDE, EDGE, CROSS, END = 0, 2, 4, 5, 6, 8, 10, 12

    class Gather:
        def __init__(self, number, buf):
            self.number, self.buf = number, buf

        def send(self, h, ia, ib, j, axis, s, group):
            along_z = (axis == "a") == (h == 0)
            to = at(s, 0, 0) if along_z else at(0, s, 0)
            ref = self.buf.at[c, block(h, ia, ib), 2 * h + j]
            remote(ref, ref, sent.at[self.number], arrived.at[self.number, group], to).start()

        def wait(self, group, count=4):
            ref = self.buf.at[c, pl.ds(0, count), 0]
            remote(ref, ref, sent.at[self.number], arrived.at[self.number, group], sibling).wait_recv()

        def over(self, places, event):
            for h in (0, 1):
                for ia, ib in places:
                    ref = self.buf.at[c, block(h, ia, ib), pl.ds(2 * h, 2)]
                    remote(ref, ref, side_sent.at[self.number], crossed.at[self.number, event], sibling).start()

        def wait_over(self, *events):
            for event in events:
                ref = self.buf.at[other, pl.ds(0, (2, 4, 4, 2, 2, 8, 4, 4, 2)[event]), pl.ds(0, 2)]
                remote(ref, ref, side_sent.at[self.number], crossed.at[self.number, event], sibling).wait_recv()

        def first(self):
            for axis, group in (("a", NEAR), ("b", OWN)):
                for turn in (0, 1):
                    for h in (0, 1):
                        for s in ways:
                            self.send(h, 0, 0, turn if s > 0 else 1 - turn, axis, s, group + turn)
            self.over([(0, 0)], 0)

        def out(self, turn):
            for h in (0, 1):
                for ia in (-1, 1):
                    for s in ways:
                        self.send(h, ia, 0, turn if ia < 0 else 1 - turn, "b", s, WIDE + turn)

        def near(self):
            self.wait(NEAR)
            for h in (0, 1):
                for s in ways:
                    self.send(h, -s, 0, 0 if s > 0 else 1, "a", s, FAR)
            self.out(0)
            self.wait(NEAR + 1)
            self.over([(-1, 0), (1, 0)], 1)

        def own(self):
            self.wait(OWN)
            for h in (0, 1):
                for s in ways:
                    self.send(h, 0, -s, 0 if s > 0 else 1, "b", s, BACK)
            self.out(1)
            self.wait(OWN + 1)
            self.over([(0, -1), (0, 1)], 2)

        def far(self):
            self.wait(FAR)
            for turn in (0, 1):
                for h in (0, 1):
                    for s in ways:
                        self.send(h, 2, 0, turn if s > 0 else 1 - turn, "b", s, CROSS + turn)
            self.over([(2, 0)], 3)

        def back(self):
            self.wait(BACK)
            self.over([(0, 2)], 4)

        def wide(self, turn):
            self.wait(WIDE + turn, 8)
            for h in (0, 1):
                for s in ways:
                    self.send(h, -s if turn == 0 else s, -s, 0 if s > 0 else 1, "b", s, EDGE + turn)
            if turn == 1:
                self.over([(-1, -1), (-1, 1), (1, -1), (1, 1)], 5)

        def cross(self):
            self.wait(CROSS)
            for h in (0, 1):
                for s in ways:
                    self.send(h, 2, -s, 0 if s > 0 else 1, "b", s, END)
            self.wait(CROSS + 1)
            self.over([(2, -1), (2, 1)], 6)

        def edge(self):
            self.wait(EDGE)
            self.wait(EDGE + 1)
            self.over([(-1, 2), (1, 2)], 7)

        def end(self):
            self.wait(END)
            self.over([(2, 2)], 8)

        def drain(self):
            ref = self.buf.at[0, pl.ds(0, self.buf.shape[1] - 1)]
            remote(ref, ref, sent.at[self.number], sent.at[self.number], sibling).wait_send()
            whole = self.buf.at[0]
            remote(whole, whole, side_sent.at[self.number], side_sent.at[self.number], sibling).wait_send()

    ups = Gather(0, up)
    downs = Gather(1, down)

    loads[0].wait()
    for q in range(QUARTERS):
        up[c, mine, q] = up_ref[:, q * piece:(q + 1) * piece].astype(jnp.bfloat16)
    pl.semaphore_wait(barrier, len(peers))
    ups.first()

    loads[1].wait()
    loads[2].wait()
    values = tok_ref[...].astype(jnp.float32)
    scale = lax.rsqrt(jnp.mean(values * values, axis=-1, keepdims=True) + epsilon)
    tok[x] = (values * scale * gain_ref[...]).astype(jnp.bfloat16)
    half = rows // 2

    def token_send(slot, part, s, group):
        ref = tok.at[slot, pl.ds(part * half, half)]
        remote(ref, ref, tok_send, tok_recv.at[group], at(0, 0, s)).start()

    def token_wait(group):
        ref = tok.at[0]
        remote(ref, ref, tok_send, tok_recv.at[group], sibling).wait_recv()

    for turn in (0, 1):
        for s in (1, -1):
            token_send(x, turn if s > 0 else 1 - turn, s, turn)
    loads[3].wait()
    for q in range(QUARTERS):
        down[c, mine, q] = down_ref[q * piece:(q + 1) * piece, :].astype(jnp.bfloat16)

    relative = (0, 1, -1, 2)

    def expand(places, begin, end, first_row, last_row):
        for h in (0, 1):
            numbers = [block(h, *place) for place in places]
            left = jnp.concatenate([
                jnp.concatenate(
                    [tok[ring(x, relative[r]), :, pl.ds(pl.multiple_of(f * share, share), share)] for f in numbers], axis=1
                ) for r in range(first_row, last_row)
            ], axis=0)
            span = slice(first_row * rows, last_row * rows)
            for core in (0, 1):
                slots = [core * QUARTERS + 2 * h + j for j in (0, 1)]
                right = jnp.concatenate([
                    jnp.concatenate([up[core, f, 2 * h + j] for f in numbers], axis=0) for j in (0, 1)
                ], axis=1)
                pre = jnp.dot(left, right, preferred_element_type=jnp.float32)
                for j, slot in enumerate(slots):
                    new = pre[:, j * piece:(j + 1) * piece]
                    if not begin:
                        new = new + acc[slot, span]
                    if end:
                        hidden[slot, span] = jnp.square(jnp.maximum(new, 0.0)).astype(jnp.bfloat16)
                    else:
                        acc[slot, span] = new

    groups = [
        [(0, 0), (-1, 0), (1, 0), (2, 0)], [(0, -1), (0, 1), (0, 2)], [(-1, -1), (-1, 1), (1, -1), (1, 1)],
        [(2, -1), (2, 1)], [(-1, 2), (1, 2), (2, 2)],
    ]

    ups.near()
    ups.own()
    ups.far()
    token_wait(0)
    for s in ways:
        token_send(ring(x, -s), 0 if s > 0 else 1, s, 2)
    ups.wide(0)
    ups.back()
    token_wait(1)
    ups.wait_over(0, 1, 3)
    expand(groups[0], True, False, 0, 3)
    ups.wait_over(2, 4)
    expand(groups[1], False, False, 0, 3)
    ups.wide(1)
    ups.cross()
    downs.first()
    ups.wait_over(5)
    expand(groups[2], False, False, 0, 3)
    token_wait(2)
    expand(groups[0], True, False, 3, 4)
    expand(groups[1], False, False, 3, 4)
    expand(groups[2], False, False, 3, 4)
    ups.edge()
    ups.wait_over(6)
    expand(groups[3], False, False, 0, 4)
    ups.end()
    ups.wait_over(7, 8)
    expand(groups[4], False, True, 0, 4)

    def spot(dz, dy):
        return ring(z, dz) * SIDE + ring(y, dy)

    def level_of(ref, unit, way, at_row):
        return ref[unit, way, at_row:at_row + 16].astype(jnp.float32)[0:1]

    def terms(shard, first, last):
        return acc[shard // 2, first:last, (shard % 2) * width:(shard % 2 + 1) * width]

    mid = rows // 2

    def one_copy(unit, way):
        span = pl.ds(0, len(units[unit]) * mid + 16)
        return remote(
            one_out.at[unit, way, span], one_in.at[unit, way, span], one_send.at[unit], one_recv.at[unit],
            at(0, 0, ways[way]),
        )

    def two_copy(unit, way):
        span = pl.ds(0, len(units[unit]) * rows + 16)
        return remote(
            two_out.at[unit, way, span], two_in.at[unit, way, span], two_send.at[unit], two_recv.at[unit],
            at(0, 0, ways[way]),
        )

    def project(first, count):
        numbers = [spot(*place) for place in shards_at[first:first + count]]
        left = jnp.concatenate([hidden[slot] for slot in range(2 * QUARTERS)], axis=1)
        right = jnp.concatenate([
            jnp.concatenate([down[core, f, q] for f in numbers], axis=1) for core in (0, 1) for q in range(QUARTERS)
        ], axis=0)
        total = jnp.dot(left, right, preferred_element_type=jnp.float32)
        for n in range(count):
            shard = first + n
            acc[shard // 2, :, (shard % 2) * width:(shard % 2 + 1) * width] = total[:, n * width:(n + 1) * width]

    def launch(unit):
        for way in (0, 1):
            first = 3 * rows + way * mid
            codes, level = encode(jnp.concatenate([terms(shard, first, first + mid) for shard in units[unit]], axis=1))
            for n, code in enumerate(codes):
                one_out[unit, way, n * mid:(n + 1) * mid] = code
            one_out[unit, way, len(codes) * mid:len(codes) * mid + 16] = level
            one_copy(unit, way).start()

    def relay(unit):
        count = len(units[unit])
        ref = one_in.at[unit, :, pl.ds(0, count * mid + 16)]
        remote(ref, ref, one_send.at[unit], one_recv.at[unit], sibling).wait_recv()
        for way in (0, 1):
            level = level_of(one_in, unit, way, count * mid)
            sums = []
            for n, shard in enumerate(units[unit]):
                taken = decode(one_in[unit, way, n * mid:(n + 1) * mid], level)
                halves = [terms(shard, (1 + way) * rows + part * mid, (1 + way) * rows + (part + 1) * mid) for part in (0, 1)]
                halves[way] = halves[way] + taken
                sums.append(jnp.concatenate(halves, axis=0))
            codes, level = encode(jnp.concatenate(sums, axis=1))
            for n, code in enumerate(codes):
                two_out[unit, way, n * rows:(n + 1) * rows] = code
            two_out[unit, way, count * rows:count * rows + 16] = level
            two_copy(unit, way).start()

    def finish(unit):
        count = len(units[unit])
        ref = two_in.at[unit, :, pl.ds(0, count * rows + 16)]
        remote(ref, ref, two_send.at[unit], two_recv.at[unit], sibling).wait_recv()
        levels = [level_of(two_in, unit, way, count * rows) for way in (0, 1)]
        for n, shard in enumerate(units[unit]):
            total = terms(shard, 0, rows)
            for way in (0, 1):
                total = total + decode(two_in[unit, way, n * rows:(n + 1) * rows], levels[way])
            f = spot(*shards_at[shard])
            out_ref[:, pl.ds(pl.multiple_of(f * width, width), width)] = total.astype(jnp.bfloat16)

    shards_at = [
        (0, 0), (-1, 0), (1, 0), (0, -1), (0, 1), (2, 0), (0, 2), (-1, -1), (-1, 1), (1, -1), (1, 1),
        (-1, 2), (2, -1), (1, 2), (2, 1), (2, 2),
    ]
    units = [(0, 1), (2, 3), (4, 5, 6), (7, 8), (9, 10), (11, 12), (13, 14), (15,)]

    downs.near()
    downs.own()
    downs.far()
    downs.wait_over(0, 1, 2)
    project(0, 4)
    launch(0)
    launch(1)
    downs.wide(0)
    downs.back()
    downs.wait_over(3, 4)
    project(4, 3)
    launch(2)
    downs.wide(1)
    relay(0)
    relay(1)
    downs.cross()
    downs.wait_over(5)
    project(7, 4)
    launch(3)
    launch(4)
    downs.edge()
    relay(2)
    downs.end()
    finish(0)
    finish(1)
    downs.wait_over(6, 7)
    project(11, 4)
    launch(5)
    launch(6)
    relay(3)
    relay(4)
    downs.wait_over(8)
    project(15, 1)
    launch(7)
    finish(2)
    for unit in (5, 6, 7):
        relay(unit)
    for unit in (3, 4, 5, 6, 7):
        finish(unit)

    ref = tok.at[pl.ds(0, 3)]
    remote(ref, ref, tok_send, tok_send, sibling).wait_send()
    for unit in range(len(units)):
        for way in (0, 1):
            one_copy(unit, way).wait_send()
            two_copy(unit, way).wait_send()
    ups.drain()
    downs.drain()


def solution(mesh):
    fs, tp = mesh.shape["fs"], mesh.shape["tp"]
    placed = (P(("fs", "tp"), None), P(), P("fs", "tp"), P("tp", "fs"))

    def whole(tokens, norm_gain, up_weight, down_weight):
        rows, depth = tokens.shape
        share, span = up_weight.shape
        width = down_weight.shape[1]
        piece = span // QUARTERS
        groups = tp // 2
        vm, dma = pltpu.VMEM, pltpu.SemaphoreType.DMA
        low, full = jnp.bfloat16, jnp.float32
        pairs = fs // 2
        return pl.pallas_call(
            kernel,
            out_shape=jax.ShapeDtypeStruct((rows, depth), low),
            in_specs=[pl.BlockSpec(memory_space=pltpu.HBM)] * 4,
            out_specs=pl.BlockSpec(memory_space=pltpu.VMEM),
            scratch_shapes=[
                vm((rows, depth), low),
                vm((1, depth), full),
                vm((share, span), full),
                vm((span, width), full),
                vm((groups, rows, depth), low),
                vm((2, fs, QUARTERS, share, piece), low),
                vm((2, fs, QUARTERS, piece, width), low),
                vm((2 * QUARTERS, groups * rows, piece), full),
                vm((2 * QUARTERS, groups * rows, piece), low),
                vm((pairs, 2, 2 * rows, LANES), low),
                vm((pairs, 2, 2 * rows, LANES), low),
                vm((pairs, 2, 4 * rows, LANES), low),
                vm((pairs, 2, 4 * rows, LANES), low),
                dma((4,)), dma, dma((3,)),
                dma((2, 13)), dma((2, 9)), dma((2,)), dma((2,)), dma((pairs,)), dma((pairs,)), dma((pairs,)), dma((pairs,)),
            ],
            compiler_params=pltpu.CompilerParams(
                collective_id=0, has_side_effects=True, vmem_limit_bytes=VMEM_LIMIT
            ),
        )(tokens, norm_gain.reshape(1, depth), up_weight, down_weight)

    return jax.shard_map(
        whole, mesh=mesh, in_specs=placed, out_specs=P(("fs", "tp"), None), check_vma=False
    )
```

```python
import functools

import jax
import jax.numpy as jnp
from jax import lax
from jax.experimental import pallas as pl
from jax.experimental.pallas import tpu as pltpu
from jax.sharding import PartitionSpec as P

epsilon = 1e-06
MESH = pl.DeviceIdType.MESH
VMEM_LIMIT = 56_020_000
SIDE = 4
QUARTERS = 4
LANES = 128
UNITS = 9
POWER = 9
PEAK = 11585.0
TINY = 1e-30


def encode(block):
    largest = jnp.max(jnp.abs(block), axis=0, keepdims=True)
    level = largest[:, :LANES]
    for start in range(LANES, block.shape[1], LANES):
        level = jnp.maximum(level, largest[:, start:start + LANES])
    level = jnp.maximum(level, TINY).astype(jnp.bfloat16)
    factor = PEAK / level.astype(jnp.float32)
    codes = []
    for start in range(0, block.shape[1], LANES):
        t = block[:, start:start + LANES] * factor
        t2 = t * t
        t4 = t2 * t2
        codes.append((t4 * t4 * t).astype(jnp.bfloat16))
    return codes, jnp.broadcast_to(level, (16, LANES))


def decode(code, level):
    y = code.astype(jnp.float32)
    size = jnp.exp(jnp.log(jnp.maximum(jnp.abs(y), 1e-38)) * (1.0 / POWER)) * (level * (1.0 / PEAK))
    return jnp.where(y > 0.0, size, jnp.where(y < 0.0, -size, 0.0))


def kernel(
    tok_hbm, gain_hbm, up_hbm, down_hbm, out_ref,
    tok_ref, gain_ref, up_ref, down_ref, tok, up, down, acc, hidden, one_out, one_in, two_out, two_in,
    load, tok_send, tok_recv, arrived, crossed, sent, side_sent, one_send, one_recv, two_send, two_recv,
):
    fs, tp = lax.axis_index("fs"), lax.axis_index("tp")
    z, y = fs // SIDE, lax.rem(fs, SIDE)
    x, c = tp // 2, lax.rem(tp, 2)
    other = 1 - c
    mine = fs
    rows = tok.shape[1]
    share = up.shape[3]
    piece = up.shape[4]
    width = down.shape[4]

    def ring(place, step):
        return lax.rem(place + (step + SIDE), SIDE)

    def at(dz, dy, dx):
        return (ring(z, dz) * SIDE + ring(y, dy), ring(x, dx) * 2 + c)

    sibling = (fs, x * 2 + other)

    def remote(src, dst, send, recv, to):
        return pltpu.make_async_remote_copy(
            src_ref=src, dst_ref=dst, send_sem=send, recv_sem=recv, device_id=to, device_id_type=MESH
        )

    barrier = pltpu.get_barrier_semaphore()
    peers = [at(1, 0, 0), at(-1, 0, 0), at(0, 1, 0), at(0, -1, 0), at(0, 0, 1), at(0, 0, -1), at(0, 0, 2), sibling]
    for to in peers:
        pl.semaphore_signal(barrier, inc=1, device_id=to, device_id_type=MESH)

    loads = [
        pltpu.make_async_copy(src, dst, load.at[n])
        for n, (src, dst) in enumerate([(up_hbm, up_ref), (tok_hbm, tok_ref), (gain_hbm, gain_ref), (down_hbm, down_ref)])
    ]
    for copy in loads:
        copy.start()

    def block(h, ia, ib):
        dz, dy = (ia, ib) if h == 0 else (ib, ia)
        return ring(z, dz) * SIDE + ring(y, dy)

    ways = (1, -1)
    NEAR, OWN, FAR, BACK, WIDE, EDGE, CROSS, END = 0, 2, 4, 5, 6, 8, 10, 12

    class Gather:
        def __init__(self, number, buf):
            self.number, self.buf = number, buf

        def send(self, h, ia, ib, j, axis, s, group):
            along_z = (axis == "a") == (h == 0)
            to = at(s, 0, 0) if along_z else at(0, s, 0)
            ref = self.buf.at[c, block(h, ia, ib), 2 * h + j]
            remote(ref, ref, sent.at[self.number], arrived.at[self.number, group], to).start()

        def wait(self, group, count=4):
            ref = self.buf.at[c, pl.ds(0, count), 0]
            remote(ref, ref, sent.at[self.number], arrived.at[self.number, group], sibling).wait_recv()

        def over(self, h, ia, ib, j, event):
            ref = self.buf.at[c, block(h, ia, ib), 2 * h + j]
            remote(ref, ref, side_sent.at[self.number], crossed.at[self.number, event], sibling).start()

        def wait_over(self, *events):
            for event in events:
                ref = self.buf.at[other, pl.ds(0, (2, 4, 4, 2, 2, 8, 4, 4, 2)[event]), pl.ds(0, 2)]
                remote(ref, ref, side_sent.at[self.number], crossed.at[self.number, event], sibling).wait_recv()

        def first(self):
            for axis, group in (("a", NEAR), ("b", OWN)):
                for turn in (0, 1):
                    for h in (0, 1):
                        for s in ways:
                            self.send(h, 0, 0, turn if s > 0 else 1 - turn, axis, s, group + turn)
            for h in (0, 1):
                for j in (0, 1):
                    self.over(h, 0, 0, j, 0)

        def out(self, turn):
            for h in (0, 1):
                for ia in (-1, 1):
                    for s in ways:
                        self.send(h, ia, 0, turn if ia < 0 else 1 - turn, "b", s, WIDE + turn)

        def near(self, turn):
            self.wait(NEAR + turn)
            if turn == 0:
                for h in (0, 1):
                    for s in ways:
                        self.send(h, -s, 0, 0 if s > 0 else 1, "a", s, FAR)
            self.out(turn)
            for h in (0, 1):
                for s in ways:
                    self.over(h, -s, 0, turn if s > 0 else 1 - turn, 1)

        def own(self, turn):
            self.wait(OWN + turn)
            if turn == 0:
                for h in (0, 1):
                    for s in ways:
                        self.send(h, 0, -s, 0 if s > 0 else 1, "b", s, BACK)
            for h in (0, 1):
                for s in ways:
                    self.over(h, 0, -s, turn if s > 0 else 1 - turn, 2)

        def far(self):
            self.wait(FAR)
            for turn in (0, 1):
                for h in (0, 1):
                    for s in ways:
                        self.send(h, 2, 0, turn if s > 0 else 1 - turn, "b", s, CROSS + turn)
            for h in (0, 1):
                for j in (0, 1):
                    self.over(h, 2, 0, j, 3)

        def back(self):
            self.wait(BACK)
            for h in (0, 1):
                for j in (0, 1):
                    self.over(h, 0, 2, j, 4)

        def wide(self, turn):
            self.wait(WIDE + turn, 8)
            for h in (0, 1):
                for s in ways:
                    self.send(h, -s if turn == 0 else s, -s, 0 if s > 0 else 1, "b", s, EDGE + turn)
            for h in (0, 1):
                for ia in (-1, 1):
                    for s in ways:
                        self.over(h, ia, -s, turn if ia < 0 else 1 - turn, 5)

        def cross(self, turn):
            self.wait(CROSS + turn)
            if turn == 0:
                for h in (0, 1):
                    for s in ways:
                        self.send(h, 2, -s, 0 if s > 0 else 1, "b", s, END)
            for h in (0, 1):
                for s in ways:
                    self.over(h, 2, -s, turn if s > 0 else 1 - turn, 6)

        def edge(self, turn):
            self.wait(EDGE + turn)
            for h in (0, 1):
                for s in ways:
                    self.over(h, -s if turn == 0 else s, 2, 0 if s > 0 else 1, 7)

        def end(self):
            self.wait(END)
            for h in (0, 1):
                for j in (0, 1):
                    self.over(h, 2, 2, j, 8)

        def drain(self):
            ref = self.buf.at[0, pl.ds(0, self.buf.shape[1] - 1)]
            remote(ref, ref, sent.at[self.number], sent.at[self.number], sibling).wait_send()
            whole = self.buf.at[0]
            remote(whole, whole, side_sent.at[self.number], side_sent.at[self.number], sibling).wait_send()

    ups = Gather(0, up)
    downs = Gather(1, down)

    loads[0].wait()
    for q in range(QUARTERS):
        up[c, mine, q] = up_ref[:, q * piece:(q + 1) * piece].astype(jnp.bfloat16)
    pl.semaphore_wait(barrier, len(peers))
    ups.first()

    loads[1].wait()
    loads[2].wait()
    values = tok_ref[...].astype(jnp.float32)
    scale = lax.rsqrt(jnp.mean(values * values, axis=-1, keepdims=True) + epsilon)
    tok[x] = (values * scale * gain_ref[...]).astype(jnp.bfloat16)
    half = rows // 2

    def token_send(slot, part, s, group):
        ref = tok.at[slot, pl.ds(part * half, half)]
        remote(ref, ref, tok_send, tok_recv.at[group], at(0, 0, s)).start()

    def token_wait(group):
        ref = tok.at[0]
        remote(ref, ref, tok_send, tok_recv.at[group], sibling).wait_recv()

    for turn in (0, 1):
        for s in (1, -1):
            token_send(x, turn if s > 0 else 1 - turn, s, turn)
    loads[3].wait()
    for q in range(QUARTERS):
        down[c, mine, q] = down_ref[q * piece:(q + 1) * piece, :].astype(jnp.bfloat16)

    relative = (0, 1, -1, 2)

    def expand(places, begin, end, first_row, last_row):
        for h in (0, 1):
            numbers = [block(h, *place) for place in places]
            left = jnp.concatenate([
                jnp.concatenate(
                    [tok[ring(x, relative[r]), :, pl.ds(pl.multiple_of(f * share, share), share)] for f in numbers], axis=1
                ) for r in range(first_row, last_row)
            ], axis=0)
            span = slice(first_row * rows, last_row * rows)
            for core in (0, 1):
                slots = [core * QUARTERS + 2 * h + j for j in (0, 1)]
                right = jnp.concatenate([
                    jnp.concatenate([up[core, f, 2 * h + j] for f in numbers], axis=0) for j in (0, 1)
                ], axis=1)
                pre = jnp.dot(left, right, preferred_element_type=jnp.float32)
                for j, slot in enumerate(slots):
                    new = pre[:, j * piece:(j + 1) * piece]
                    if not begin:
                        new = new + acc[slot, span]
                    if end:
                        hidden[slot, span] = jnp.square(jnp.maximum(new, 0.0)).astype(jnp.bfloat16)
                    else:
                        acc[slot, span] = new

    groups = [
        [(0, 0), (-1, 0), (1, 0), (2, 0)], [(-1, -1), (-1, 1), (1, -1), (1, 1)], [(0, -1), (0, 1)],
        [(2, -1), (2, 1)], [(-1, 2), (1, 2)], [(0, 2), (2, 2)],
    ]

    ups.near(0)
    ups.near(1)
    ups.own(0)
    ups.own(1)
    ups.far()
    token_wait(0)
    for s in ways:
        token_send(ring(x, -s), 0 if s > 0 else 1, s, 2)
    ups.wide(0)
    token_wait(1)
    ups.wait_over(0, 1, 3)
    expand(groups[0], True, False, 0, 3)
    ups.wide(1)
    ups.back()
    ups.wait_over(5)
    expand(groups[1], False, False, 0, 3)
    ups.cross(0)
    ups.wait_over(2)
    expand(groups[2], False, False, 0, 3)
    ups.cross(1)
    downs.first()
    token_wait(2)
    expand(groups[0], True, False, 3, 4)
    expand(groups[1], False, False, 3, 4)
    expand(groups[2], False, False, 3, 4)
    ups.edge(0)
    ups.edge(1)
    ups.wait_over(6)
    expand(groups[3], False, False, 0, 4)
    ups.end()
    ups.wait_over(7)
    expand(groups[4], False, False, 0, 4)
    downs.near(0)
    ups.wait_over(4, 8)
    expand(groups[5], False, True, 0, 4)

    def spot(dz, dy):
        return ring(z, dz) * SIDE + ring(y, dy)

    def level_of(ref, unit, way, at_row):
        return ref[unit, way, at_row:at_row + 16].astype(jnp.float32)[0:1]

    def terms(shard, first, last):
        return acc[shard // 2, first:last, (shard % 2) * width:(shard % 2 + 1) * width]

    mid = rows // 2

    def one_copy(unit, way):
        span = pl.ds(0, len(units[unit]) * mid + 16)
        return remote(
            one_out.at[unit, way, span], one_in.at[unit, way, span], one_send.at[unit], one_recv.at[unit],
            at(0, 0, ways[way]),
        )

    def far_copy(unit):
        span = pl.ds(0, len(units[unit]) * rows + 16)
        return remote(
            one_out.at[unit, 0, span], one_in.at[unit, 0, span], one_send.at[unit], one_recv.at[unit], at(0, 0, 2)
        )

    def two_copy(unit, way):
        span = pl.ds(0, len(units[unit]) * rows + 16)
        return remote(
            two_out.at[unit, way, span], two_in.at[unit, way, span], two_send.at[unit], two_recv.at[unit],
            at(0, 0, ways[way]),
        )

    def project(first, count):
        numbers = [spot(*place) for place in shards_at[first:first + count]]
        right = jnp.concatenate([
            jnp.concatenate([down[core, f, q] for f in numbers], axis=1) for core in (0, 1) for q in range(QUARTERS)
        ], axis=0)
        parts = 1 if count > 2 else 2
        tall = 4 * rows // parts
        for part in range(parts):
            span = slice(part * tall, (part + 1) * tall)
            left = jnp.concatenate([hidden[slot, span] for slot in range(2 * QUARTERS)], axis=1)
            total = jnp.dot(left, right, preferred_element_type=jnp.float32)
            for n in range(count):
                shard = first + n
                acc[shard // 2, span, (shard % 2) * width:(shard % 2 + 1) * width] = total[:, n * width:(n + 1) * width]

    def pack(ref, unit, way, codes, level):
        tall = codes[0].shape[0]
        for n, code in enumerate(codes):
            ref[unit, way, n * tall:(n + 1) * tall] = code
        ref[unit, way, len(codes) * tall:len(codes) * tall + 16] = level

    def gather_terms(unit, first, last):
        return jnp.concatenate([terms(shard, first, last) for shard in units[unit]], axis=1)

    def launch(unit):
        if unit in direct:
            pack(one_out, unit, 0, *encode(gather_terms(unit, 3 * rows, 4 * rows)))
            far_copy(unit).start()
            for way in (0, 1):
                pack(two_out, unit, way, *encode(gather_terms(unit, (1 + way) * rows, (2 + way) * rows)))
                two_copy(unit, way).start()
        else:
            for way in (0, 1):
                first = 3 * rows + way * mid
                pack(one_out, unit, way, *encode(gather_terms(unit, first, first + mid)))
                one_copy(unit, way).start()

    def relay(unit):
        count = len(units[unit])
        ref = one_in.at[unit, :, pl.ds(0, count * mid + 16)]
        remote(ref, ref, one_send.at[unit], one_recv.at[unit], sibling).wait_recv()
        for way in (0, 1):
            level = level_of(one_in, unit, way, count * mid)
            sums = []
            for n, shard in enumerate(units[unit]):
                taken = decode(one_in[unit, way, n * mid:(n + 1) * mid], level)
                halves = [terms(shard, (1 + way) * rows + part * mid, (1 + way) * rows + (part + 1) * mid) for part in (0, 1)]
                halves[way] = halves[way] + taken
                sums.append(jnp.concatenate(halves, axis=0))
            pack(two_out, unit, way, *encode(jnp.concatenate(sums, axis=1)))
            two_copy(unit, way).start()

    def finish(unit):
        count = len(units[unit])
        ref = two_in.at[unit, :, pl.ds(0, count * rows + 16)]
        remote(ref, ref, two_send.at[unit], two_recv.at[unit], sibling).wait_recv()
        incoming = [(two_in, 0), (two_in, 1)]
        if unit in direct:
            far_copy(unit).wait_recv()
            incoming.append((one_in, 0))
        levels = [level_of(buf, unit, way, count * rows) for buf, way in incoming]
        for n, shard in enumerate(units[unit]):
            total = terms(shard, 0, rows)
            for (buf, way), level in zip(incoming, levels):
                total = total + decode(buf[unit, way, n * rows:(n + 1) * rows], level)
            f = spot(*shards_at[shard])
            out_ref[:, pl.ds(pl.multiple_of(f * width, width), width)] = total.astype(jnp.bfloat16)

    shards_at = [
        (0, 0), (-1, 0), (1, 0), (0, -1), (0, 1), (-1, -1), (-1, 1), (1, -1), (1, 1), (2, 0), (0, 2),
        (-1, 2), (2, -1), (1, 2), (2, 1), (2, 2),
    ]
    units = [(0,), (1, 2), (3, 4), (5, 6), (7, 8), (9, 10), (11, 12), (13, 14), (15,)]
    direct = (0, 1, 2)

    downs.near(1)
    downs.wait_over(0)
    project(0, 1)
    launch(0)
    downs.own(0)
    downs.own(1)
    downs.far()
    downs.wait_over(1, 2)
    project(1, 4)
    launch(1)
    launch(2)
    downs.wide(0)
    downs.wide(1)
    finish(0)
    downs.wait_over(5)
    project(5, 4)
    launch(3)
    launch(4)
    downs.back()
    downs.wait_over(3, 4)
    project(9, 2)
    launch(5)
    downs.cross(0)
    downs.cross(1)
    downs.edge(0)
    relay(3)
    relay(4)
    downs.edge(1)
    finish(1)
    finish(2)
    downs.wait_over(6, 7)
    project(11, 4)
    launch(6)
    launch(7)
    if 5 not in direct:
        relay(5)
    downs.end()
    downs.wait_over(8)
    project(15, 1)
    launch(8)
    for unit in (6, 7, 8):
        if unit not in direct:
            relay(unit)
    for unit in (3, 4, 5, 6, 7, 8):
        finish(unit)

    ref = tok.at[pl.ds(0, 3)]
    remote(ref, ref, tok_send, tok_send, sibling).wait_send()
    for unit in range(len(units)):
        for way in (0, 1):
            two_copy(unit, way).wait_send()
            if unit not in direct:
                one_copy(unit, way).wait_send()
        if unit in direct:
            far_copy(unit).wait_send()
    ups.drain()
    downs.drain()


def solution(mesh):
    fs, tp = mesh.shape["fs"], mesh.shape["tp"]
    placed = (P(("fs", "tp"), None), P(), P("fs", "tp"), P("tp", "fs"))

    def whole(tokens, norm_gain, up_weight, down_weight):
        rows, depth = tokens.shape
        share, span = up_weight.shape
        width = down_weight.shape[1]
        piece = span // QUARTERS
        groups = tp // 2
        vm, dma = pltpu.VMEM, pltpu.SemaphoreType.DMA
        low, full = jnp.bfloat16, jnp.float32
        return pl.pallas_call(
            kernel,
            out_shape=jax.ShapeDtypeStruct((rows, depth), low),
            in_specs=[pl.BlockSpec(memory_space=pltpu.HBM)] * 4,
            out_specs=pl.BlockSpec(memory_space=pltpu.VMEM),
            scratch_shapes=[
                vm((rows, depth), low),
                vm((1, depth), full),
                vm((share, span), full),
                vm((span, width), full),
                vm((groups, rows, depth), low),
                vm((2, fs, QUARTERS, share, piece), low),
                vm((2, fs, QUARTERS, piece, width), low),
                vm((2 * QUARTERS, groups * rows, piece), full),
                vm((2 * QUARTERS, groups * rows, piece), low),
                vm((UNITS, 2, 2 * rows + 16, LANES), low),
                vm((UNITS, 2, 2 * rows + 16, LANES), low),
                vm((UNITS, 2, 2 * rows + 16, LANES), low),
                vm((UNITS, 2, 2 * rows + 16, LANES), low),
                dma((4,)), dma, dma((3,)),
                dma((2, 13)), dma((2, 9)), dma((2,)), dma((2,)), dma((UNITS,)), dma((UNITS,)), dma((UNITS,)), dma((UNITS,)),
            ],
            compiler_params=pltpu.CompilerParams(
                collective_id=0, has_side_effects=True, vmem_limit_bytes=VMEM_LIMIT
            ),
        )(tokens, norm_gain.reshape(1, depth), up_weight, down_weight)

    return jax.shard_map(
        whole, mesh=mesh, in_specs=placed, out_specs=P(("fs", "tp"), None), check_vma=False
    )
```

```python
import functools

import jax
import jax.numpy as jnp
from jax import lax
from jax.experimental import pallas as pl
from jax.experimental.pallas import tpu as pltpu
from jax.sharding import PartitionSpec as P

epsilon = 1e-06
MESH = pl.DeviceIdType.MESH
VMEM_LIMIT = 48_000_000
SIDE = 4
QUARTERS = 4
LANES = 128
UNITS = 9
POWER = 9
PEAK = 11585.0
TINY = 1e-30


def encode(block):
    largest = jnp.max(jnp.abs(block), axis=0, keepdims=True)
    level = largest[:, :LANES]
    for start in range(LANES, block.shape[1], LANES):
        level = jnp.maximum(level, largest[:, start:start + LANES])
    level = jnp.maximum(level, TINY).astype(jnp.bfloat16)
    factor = PEAK / level.astype(jnp.float32)
    codes = []
    for start in range(0, block.shape[1], LANES):
        t = block[:, start:start + LANES] * factor
        t2 = t * t
        t4 = t2 * t2
        codes.append((t4 * t4 * t).astype(jnp.bfloat16))
    return codes, jnp.broadcast_to(level, (8, LANES))


def decode(code, level):
    y = code.astype(jnp.float32)
    size = jnp.exp(jnp.log(jnp.maximum(jnp.abs(y), 1e-38)) * (1.0 / POWER)) * (level * (1.0 / PEAK))
    return jnp.where(y > 0.0, size, jnp.where(y < 0.0, -size, 0.0))


def kernel(
    tok_hbm, gain_hbm, up_hbm, down_hbm, out_ref,
    tok_ref, gain_ref, up_ref, down_ref, tok, up, down, acc, hidden, one_out, one_in, two_out, two_in,
    load, tok_send, tok_recv, arrived, crossed, sent, side_sent, one_send, one_recv, two_send, two_recv,
):
    fs, tp = lax.axis_index("fs"), lax.axis_index("tp")
    z, y = fs // SIDE, lax.rem(fs, SIDE)
    x, c = tp // 2, lax.rem(tp, 2)
    other = 1 - c
    mine = fs
    rows = tok.shape[1]
    share = up.shape[3]
    piece = up.shape[4]
    width = down.shape[4]

    def ring(place, step):
        return lax.rem(place + (step + SIDE), SIDE)

    def at(dz, dy, dx):
        return (ring(z, dz) * SIDE + ring(y, dy), ring(x, dx) * 2 + c)

    sibling = (fs, x * 2 + other)

    def remote(src, dst, send, recv, to):
        return pltpu.make_async_remote_copy(
            src_ref=src, dst_ref=dst, send_sem=send, recv_sem=recv, device_id=to, device_id_type=MESH
        )

    barrier = pltpu.get_barrier_semaphore()
    peers = [at(1, 0, 0), at(-1, 0, 0), at(0, 1, 0), at(0, -1, 0), at(0, 0, 1), at(0, 0, -1), at(0, 0, 2), sibling]
    for to in peers:
        pl.semaphore_signal(barrier, inc=1, device_id=to, device_id_type=MESH)

    loads = [
        pltpu.make_async_copy(src, dst, load.at[n])
        for n, (src, dst) in enumerate([(up_hbm, up_ref), (tok_hbm, tok_ref), (gain_hbm, gain_ref), (down_hbm, down_ref)])
    ]
    for copy in loads:
        copy.start()

    def block(h, ia, ib):
        dz, dy = (ia, ib) if h == 0 else (ib, ia)
        return ring(z, dz) * SIDE + ring(y, dy)

    ways = (1, -1)
    NEAR, OWN, FAR, BACK, WIDE, MID, LATE, END = 0, 2, 4, 5, 6, 8, 10, 12

    class Gather:
        def __init__(self, number, buf, skew):
            self.number, self.buf, self.skew = number, buf, skew

        def send(self, h, ia, ib, j, axis, s, group):
            along_z = (axis == "a") == (h == 0)
            to = at(s, 0, 0) if along_z else at(0, s, 0)
            ref = self.buf.at[c, block(h, ia, ib), 2 * h + j]
            remote(ref, ref, sent.at[self.number], arrived.at[self.number, group], to).start()

        def wait(self, group, count=4):
            ref = self.buf.at[c, pl.ds(0, count), 0]
            remote(ref, ref, sent.at[self.number], arrived.at[self.number, group], sibling).wait_recv()

        def over(self, h, ia, ib, j, event):
            ref = self.buf.at[c, block(h, ia, ib), 2 * h + j]
            remote(ref, ref, side_sent.at[self.number], crossed.at[self.number, event], sibling).start()

        def wait_over(self, *events):
            for event in events:
                ref = self.buf.at[other, pl.ds(0, (2, 4, 4, 2, 2, 8, 4, 4, 2)[event]), pl.ds(0, 2)]
                remote(ref, ref, side_sent.at[self.number], crossed.at[self.number, event], sibling).wait_recv()

        def first(self):
            for axis, group in (("a", NEAR), ("b", OWN)):
                for turn in (0, 1):
                    for h in (0, 1):
                        for s in ways:
                            self.send(h, 0, 0, turn if s > 0 else 1 - turn, axis, s, group + turn)
            for h in (0, 1):
                for j in (0, 1):
                    self.over(h, 0, 0, j, 0)

        def out(self, turn):
            for h in (0, 1):
                for ia in (-1, 1):
                    for s in ways:
                        self.send(h, ia, 0, turn if ia < 0 else 1 - turn, "b", s, WIDE + turn)

        def near(self, turn):
            self.wait(NEAR + turn)
            if turn == 0:
                for h in (0, 1):
                    for s in ways:
                        self.send(h, -s, 0, 0 if s > 0 else 1, "a", s, FAR)
            self.out(turn)
            for h in (0, 1):
                for s in ways:
                    self.over(h, -s, 0, turn if s > 0 else 1 - turn, 1)

        def own(self, turn):
            self.wait(OWN + turn)
            if turn == 0:
                for h in (0, 1):
                    for s in ways:
                        self.send(h, 0, -s, 0 if s > 0 else 1, "b", s, BACK)
            for h in (0, 1):
                for s in ways:
                    self.over(h, 0, -s, turn if s > 0 else 1 - turn, 2)

        def out_far(self, h, turn):
            group = LATE + 1 if h == 1 and turn == 1 and self.skew else MID + turn
            for s in ways:
                self.send(h, 2, 0, turn if s > 0 else 1 - turn, "b", s, group)

        def far(self):
            self.wait(FAR)
            for turn in (0, 1):
                for h in (0, 1):
                    if h == 0 or turn == 0 or not self.skew:
                        self.out_far(h, turn)
            for h in (0, 1):
                for j in (0, 1):
                    self.over(h, 2, 0, j, 3)

        def back(self):
            self.wait(BACK)
            for h in (0, 1):
                for j in (0, 1):
                    self.over(h, 0, 2, j, 4)

        def wide(self, turn):
            self.wait(WIDE + turn, 8)
            for h in (0, 1):
                for s in ways:
                    ia = -s if turn == 0 else s
                    group = (MID + 1, LATE)[turn] if h == 1 and self.skew else LATE + turn
                    self.send(h, ia, -s, 0 if s > 0 else 1, "b", s, group)
            if turn == 1 and self.skew:
                self.out_far(1, 1)
            for h in (0, 1):
                for ia in (-1, 1):
                    for s in ways:
                        self.over(h, ia, -s, turn if ia < 0 else 1 - turn, 5)

        def crossed_far(self, h, turn, event):
            if turn == 0:
                for s in ways:
                    self.send(h, 2, -s, 0 if s > 0 else 1, "b", s, END)
            for s in ways:
                self.over(h, 2, -s, turn if s > 0 else 1 - turn, event)

        def crossed_edge(self, h, turn, event):
            for s in ways:
                self.over(h, -s if turn == 0 else s, 2, 0 if s > 0 else 1, event)

        def mid(self, turn):
            self.wait(MID + turn)
            self.crossed_far(0, turn, 6)
            if not self.skew:
                self.crossed_far(1, turn, 6)
            elif turn == 0:
                self.crossed_far(1, 0, 7)
            else:
                self.crossed_edge(1, 0, 6)

        def late(self, turn):
            self.wait(LATE + turn)
            self.crossed_edge(0, turn, 7)
            if not self.skew:
                self.crossed_edge(1, turn, 7)
            elif turn == 0:
                self.crossed_edge(1, 1, 6)
            else:
                self.crossed_far(1, 1, 7)

        def end(self):
            self.wait(END)
            for h in (0, 1):
                for j in (0, 1):
                    self.over(h, 2, 2, j, 8)

        def drain(self):
            ref = self.buf.at[0, pl.ds(0, self.buf.shape[1] - 1)]
            remote(ref, ref, sent.at[self.number], sent.at[self.number], sibling).wait_send()
            whole = self.buf.at[0]
            remote(whole, whole, side_sent.at[self.number], side_sent.at[self.number], sibling).wait_send()

    ups = Gather(0, up, False)
    downs = Gather(1, down, True)

    loads[0].wait()
    for q in range(QUARTERS):
        up[c, mine, q] = up_ref[:, q * piece:(q + 1) * piece].astype(jnp.bfloat16)
    pl.semaphore_wait(barrier, len(peers))
    ups.first()

    loads[1].wait()
    loads[2].wait()
    values = tok_ref[...].astype(jnp.float32)
    scale = lax.rsqrt(jnp.mean(values * values, axis=-1, keepdims=True) + epsilon)
    tok[x] = (values * scale * gain_ref[...]).astype(jnp.bfloat16)
    half = rows // 2

    def token_send(slot, part, s, group):
        ref = tok.at[slot, pl.ds(part * half, half)]
        remote(ref, ref, tok_send, tok_recv.at[group], at(0, 0, s)).start()

    def token_wait(group):
        ref = tok.at[0]
        remote(ref, ref, tok_send, tok_recv.at[group], sibling).wait_recv()

    for turn in (0, 1):
        for s in (1, -1):
            token_send(x, turn if s > 0 else 1 - turn, s, turn)
    loads[3].wait()
    for q in range(QUARTERS):
        down[c, mine, q] = down_ref[q * piece:(q + 1) * piece, :].astype(jnp.bfloat16)

    relative = (0, 1, -1, 2)

    def expand(places, begin, end, first_row, last_row):
        for h in (0, 1):
            numbers = [block(h, *place) for place in places]
            left = jnp.concatenate([
                jnp.concatenate(
                    [tok[ring(x, relative[r]), :, pl.ds(pl.multiple_of(f * share, share), share)] for f in numbers], axis=1
                ) for r in range(first_row, last_row)
            ], axis=0)
            span = slice(first_row * rows, last_row * rows)
            for core in (0, 1):
                slots = [core * QUARTERS + 2 * h + j for j in (0, 1)]
                right = jnp.concatenate([
                    jnp.concatenate([up[core, f, 2 * h + j] for f in numbers], axis=0) for j in (0, 1)
                ], axis=1)
                pre = jnp.dot(left, right, preferred_element_type=jnp.float32)
                for j, slot in enumerate(slots):
                    new = pre[:, j * piece:(j + 1) * piece]
                    if not begin:
                        new = new + acc[slot, span]
                    if end:
                        hidden[slot, span] = jnp.square(jnp.maximum(new, 0.0)).astype(jnp.bfloat16)
                    else:
                        acc[slot, span] = new

    groups = [
        [(0, 0), (-1, 0), (1, 0), (2, 0)], [(-1, -1), (-1, 1), (1, -1), (1, 1)], [(0, -1), (0, 1)],
        [(2, -1), (2, 1)], [(-1, 2), (1, 2)], [(0, 2), (2, 2)],
    ]

    ups.near(0)
    ups.near(1)
    ups.own(0)
    ups.own(1)
    ups.far()
    token_wait(0)
    for s in ways:
        token_send(ring(x, -s), 0 if s > 0 else 1, s, 2)
    ups.wide(0)
    token_wait(1)
    ups.wait_over(0, 1, 3)
    expand(groups[0], True, False, 0, 3)
    ups.wide(1)
    ups.back()
    ups.wait_over(5)
    expand(groups[1], False, False, 0, 3)
    ups.mid(0)
    ups.wait_over(2)
    expand(groups[2], False, False, 0, 3)
    ups.mid(1)
    downs.first()
    token_wait(2)
    expand(groups[0], True, False, 3, 4)
    expand(groups[1], False, False, 3, 4)
    expand(groups[2], False, False, 3, 4)
    ups.late(0)
    ups.late(1)
    ups.wait_over(6)
    expand(groups[3], False, False, 0, 4)
    ups.end()
    ups.wait_over(7)
    expand(groups[4], False, False, 0, 4)
    downs.near(0)
    ups.wait_over(4, 8)
    expand(groups[5], False, True, 0, 4)

    def spot(dz, dy):
        return ring(z, dz) * SIDE + ring(y, dy)

    def level_of(ref, unit, way, at_row):
        return ref[unit, way, at_row:at_row + 8].astype(jnp.float32)[0:1]

    def terms(shard, first, last):
        return acc[shard // 2, first:last, (shard % 2) * width:(shard % 2 + 1) * width]

    mid = rows // 2

    def one_copy(unit, way):
        span = pl.ds(0, len(units[unit]) * mid + 8)
        return remote(
            one_out.at[unit, way, span], one_in.at[unit, way, span], one_send.at[unit], one_recv.at[unit],
            at(0, 0, ways[way]),
        )

    def far_copy(unit):
        span = pl.ds(0, len(units[unit]) * rows + 8)
        return remote(
            one_out.at[unit, 0, span], one_in.at[unit, 0, span], one_send.at[unit], one_recv.at[unit], at(0, 0, 2)
        )

    def two_copy(unit, way):
        span = pl.ds(0, len(units[unit]) * rows + 8)
        return remote(
            two_out.at[unit, way, span], two_in.at[unit, way, span], two_send.at[unit], two_recv.at[unit],
            at(0, 0, ways[way]),
        )

    def project(first, count):
        numbers = [spot(*place) for place in shards_at[first:first + count]]
        right = jnp.concatenate([
            jnp.concatenate([down[core, f, q] for f in numbers], axis=1) for core in (0, 1) for q in range(QUARTERS)
        ], axis=0)
        parts = 1 if count > 2 else 2
        tall = 4 * rows // parts
        for part in range(parts):
            span = slice(part * tall, (part + 1) * tall)
            left = jnp.concatenate([hidden[slot, span] for slot in range(2 * QUARTERS)], axis=1)
            total = jnp.dot(left, right, preferred_element_type=jnp.float32)
            for n in range(count):
                shard = first + n
                acc[shard // 2, span, (shard % 2) * width:(shard % 2 + 1) * width] = total[:, n * width:(n + 1) * width]

    def pack(ref, unit, way, codes, level):
        tall = codes[0].shape[0]
        for n, code in enumerate(codes):
            ref[unit, way, n * tall:(n + 1) * tall] = code
        ref[unit, way, len(codes) * tall:len(codes) * tall + 8] = level

    def gather_terms(unit, first, last):
        return jnp.concatenate([terms(shard, first, last) for shard in units[unit]], axis=1)

    def launch(unit):
        if unit in direct:
            pack(one_out, unit, 0, *encode(gather_terms(unit, 3 * rows, 4 * rows)))
            far_copy(unit).start()
            for way in (0, 1):
                pack(two_out, unit, way, *encode(gather_terms(unit, (1 + way) * rows, (2 + way) * rows)))
                two_copy(unit, way).start()
        else:
            for way in (0, 1):
                first = 3 * rows + way * mid
                pack(one_out, unit, way, *encode(gather_terms(unit, first, first + mid)))
                one_copy(unit, way).start()

    def relay(unit):
        count = len(units[unit])
        ref = one_in.at[unit, :, pl.ds(0, count * mid + 8)]
        remote(ref, ref, one_send.at[unit], one_recv.at[unit], sibling).wait_recv()
        for way in (0, 1):
            level = level_of(one_in, unit, way, count * mid)
            sums = []
            for n, shard in enumerate(units[unit]):
                taken = decode(one_in[unit, way, n * mid:(n + 1) * mid], level)
                halves = [terms(shard, (1 + way) * rows + part * mid, (1 + way) * rows + (part + 1) * mid) for part in (0, 1)]
                halves[way] = halves[way] + taken
                sums.append(jnp.concatenate(halves, axis=0))
            pack(two_out, unit, way, *encode(jnp.concatenate(sums, axis=1)))
            two_copy(unit, way).start()

    def finish(unit):
        count = len(units[unit])
        ref = two_in.at[unit, :, pl.ds(0, count * rows + 8)]
        remote(ref, ref, two_send.at[unit], two_recv.at[unit], sibling).wait_recv()
        incoming = [(two_in, 0), (two_in, 1)]
        if unit in direct:
            far_copy(unit).wait_recv()
            incoming.append((one_in, 0))
        levels = [level_of(buf, unit, way, count * rows) for buf, way in incoming]
        for n, shard in enumerate(units[unit]):
            total = terms(shard, 0, rows)
            for (buf, way), level in zip(incoming, levels):
                total = total + decode(buf[unit, way, n * rows:(n + 1) * rows], level)
            f = spot(*shards_at[shard])
            out_ref[:, pl.ds(pl.multiple_of(f * width, width), width)] = total.astype(jnp.bfloat16)

    shards_at = [
        (0, 0), (-1, 0), (1, 0), (0, -1), (0, 1), (-1, -1), (-1, 1), (1, -1), (1, 1), (2, 0), (0, 2),
        (2, -1), (2, 1), (-1, 2), (1, 2), (2, 2),
    ]
    units = [(0,), (1, 2), (3, 4), (5, 6), (7, 8), (9, 10), (11, 12), (13, 14), (15,)]
    direct = (0, 1, 2, 5)

    downs.near(1)
    downs.wait_over(0)
    project(0, 1)
    launch(0)
    downs.own(0)
    downs.own(1)
    downs.far()
    downs.wait_over(1, 2)
    project(1, 4)
    launch(1)
    launch(2)
    downs.wide(0)
    downs.wide(1)
    finish(0)
    downs.wait_over(5)
    project(5, 4)
    launch(3)
    launch(4)
    downs.back()
    downs.mid(0)
    downs.wait_over(3, 4)
    project(9, 2)
    launch(5)
    downs.mid(1)
    downs.late(0)
    relay(3)
    relay(4)
    downs.wait_over(6)
    project(11, 2)
    launch(6)
    downs.late(1)
    finish(1)
    finish(2)
    downs.end()
    if 5 not in direct:
        relay(5)
    downs.wait_over(7)
    project(13, 2)
    launch(7)
    downs.wait_over(8)
    project(15, 1)
    launch(8)
    for unit in (6, 7, 8):
        if unit not in direct:
            relay(unit)
    for unit in (3, 4, 5, 6, 7, 8):
        finish(unit)

    ref = tok.at[pl.ds(0, 3)]
    remote(ref, ref, tok_send, tok_send, sibling).wait_send()
    for unit in range(len(units)):
        for way in (0, 1):
            two_copy(unit, way).wait_send()
            if unit not in direct:
                one_copy(unit, way).wait_send()
        if unit in direct:
            far_copy(unit).wait_send()
    ups.drain()
    downs.drain()


def solution(mesh):
    fs, tp = mesh.shape["fs"], mesh.shape["tp"]
    placed = (P(("fs", "tp"), None), P(), P("fs", "tp"), P("tp", "fs"))

    def whole(tokens, norm_gain, up_weight, down_weight):
        rows, depth = tokens.shape
        share, span = up_weight.shape
        width = down_weight.shape[1]
        piece = span // QUARTERS
        groups = tp // 2
        vm, dma = pltpu.VMEM, pltpu.SemaphoreType.DMA
        low, full = jnp.bfloat16, jnp.float32
        return pl.pallas_call(
            kernel,
            out_shape=jax.ShapeDtypeStruct((rows, depth), low),
            in_specs=[pl.BlockSpec(memory_space=pltpu.HBM)] * 4,
            out_specs=pl.BlockSpec(memory_space=pltpu.VMEM),
            scratch_shapes=[
                vm((rows, depth), low),
                vm((1, depth), full),
                vm((share, span), full),
                vm((span, width), full),
                vm((groups, rows, depth), low),
                vm((2, fs, QUARTERS, share, piece), low),
                vm((2, fs, QUARTERS, piece, width), low),
                vm((2 * QUARTERS, groups * rows, piece), full),
                vm((2 * QUARTERS, groups * rows, piece), low),
                vm((UNITS, 2, 2 * rows + 8, LANES), low),
                vm((UNITS, 2, 2 * rows + 8, LANES), low),
                vm((UNITS, 2, 2 * rows + 8, LANES), low),
                vm((UNITS, 2, 2 * rows + 8, LANES), low),
                dma((4,)), dma, dma((3,)),
                dma((2, 13)), dma((2, 9)), dma((2,)), dma((2,)), dma((UNITS,)), dma((UNITS,)), dma((UNITS,)), dma((UNITS,)),
            ],
            compiler_params=pltpu.CompilerParams(
                collective_id=0, has_side_effects=True, vmem_limit_bytes=VMEM_LIMIT
            ),
        )(*(
            pltpu.with_memory_space_constraint(array, pltpu.HBM)
            for array in (tokens, norm_gain.reshape(1, depth), up_weight, down_weight)
        ))

    return jax.shard_map(
        whole, mesh=mesh, in_specs=placed, out_specs=P(("fs", "tp"), None), check_vma=False
    )
```

```python
import functools

import jax
import jax.numpy as jnp
from jax import lax
from jax.experimental import pallas as pl
from jax.experimental.pallas import tpu as pltpu
from jax.sharding import PartitionSpec as P

epsilon = 1e-06
MESH = pl.DeviceIdType.MESH
VMEM_LIMIT = 48_000_000
SIDE = 4
QUARTERS = 4
LANES = 128
UNITS = 9
POWER = 9
PEAK = 11585.0
TINY = 1e-30


def encode(block):
    largest = jnp.max(jnp.abs(block), axis=0, keepdims=True)
    level = largest[:, :LANES]
    for start in range(LANES, block.shape[1], LANES):
        level = jnp.maximum(level, largest[:, start:start + LANES])
    level = jnp.maximum(level, TINY).astype(jnp.bfloat16)
    factor = PEAK / level.astype(jnp.float32)
    codes = []
    for start in range(0, block.shape[1], LANES):
        t = block[:, start:start + LANES] * factor
        t2 = t * t
        t4 = t2 * t2
        codes.append((t4 * t4 * t).astype(jnp.bfloat16))
    return codes, jnp.broadcast_to(level, (8, LANES))


def decode(code, level):
    y = code.astype(jnp.float32)
    size = jnp.exp(jnp.log(jnp.maximum(jnp.abs(y), 1e-38)) * (1.0 / POWER)) * (level * (1.0 / PEAK))
    return jnp.where(y > 0.0, size, jnp.where(y < 0.0, -size, 0.0))


def kernel(
    tok_hbm, gain_hbm, up_hbm, down_hbm, out_ref,
    tok_ref, gain_ref, up_ref, down_ref, tok, up, down, acc, hidden, one_out, one_in, two_out, two_in,
    load, tok_send, tok_recv, arrived, crossed, sent, side_sent, one_send, one_recv, two_send, two_recv,
):
    fs, tp = lax.axis_index("fs"), lax.axis_index("tp")
    z, y = fs // SIDE, lax.rem(fs, SIDE)
    x, c = tp // 2, lax.rem(tp, 2)
    other = 1 - c
    mine = fs
    rows = tok.shape[1]
    share = up.shape[3]
    piece = up.shape[4]
    width = down.shape[4]

    def ring(place, step):
        return lax.rem(place + (step + SIDE), SIDE)

    def at(dz, dy, dx):
        return (ring(z, dz) * SIDE + ring(y, dy), ring(x, dx) * 2 + c)

    sibling = (fs, x * 2 + other)

    def remote(src, dst, send, recv, to):
        return pltpu.make_async_remote_copy(
            src_ref=src, dst_ref=dst, send_sem=send, recv_sem=recv, device_id=to, device_id_type=MESH
        )

    barrier = pltpu.get_barrier_semaphore()
    peers = [at(1, 0, 0), at(-1, 0, 0), at(0, 1, 0), at(0, -1, 0), at(0, 0, 1), at(0, 0, -1), at(0, 0, 2), sibling]
    for to in peers:
        pl.semaphore_signal(barrier, inc=1, device_id=to, device_id_type=MESH)

    loads = [
        pltpu.make_async_copy(src, dst, load.at[n])
        for n, (src, dst) in enumerate([(up_hbm, up_ref), (tok_hbm, tok_ref), (gain_hbm, gain_ref), (down_hbm, down_ref)])
    ]
    for copy in loads:
        copy.start()

    def block(h, ia, ib):
        dz, dy = (ia, ib) if h == 0 else (ib, ia)
        return ring(z, dz) * SIDE + ring(y, dy)

    ways = (1, -1)
    NEAR, OWN, FAR, BACK, WIDE, MID, LATE, END = 0, 2, 4, 5, 6, 8, 10, 12

    class Gather:
        def __init__(self, number, buf, skew):
            self.number, self.buf, self.skew = number, buf, skew

        def send(self, h, ia, ib, j, axis, s, group):
            along_z = (axis == "a") == (h == 0)
            to = at(s, 0, 0) if along_z else at(0, s, 0)
            ref = self.buf.at[c, block(h, ia, ib), 2 * h + j]
            remote(ref, ref, sent.at[self.number], arrived.at[self.number, group], to).start()

        def wait(self, group, count=4):
            ref = self.buf.at[c, pl.ds(0, count), 0]
            remote(ref, ref, sent.at[self.number], arrived.at[self.number, group], sibling).wait_recv()

        def over(self, h, ia, ib, j, event):
            ref = self.buf.at[c, block(h, ia, ib), 2 * h + j]
            remote(ref, ref, side_sent.at[self.number], crossed.at[self.number, event], sibling).start()

        def wait_over(self, *events):
            for event in events:
                ref = self.buf.at[other, pl.ds(0, (2, 4, 4, 2, 2, 8, 4, 4, 2)[event]), pl.ds(0, 2)]
                remote(ref, ref, side_sent.at[self.number], crossed.at[self.number, event], sibling).wait_recv()

        def first(self):
            for axis, group in (("a", NEAR), ("b", OWN)):
                for turn in (0, 1):
                    for h in (0, 1):
                        for s in ways:
                            self.send(h, 0, 0, turn if s > 0 else 1 - turn, axis, s, group + turn)
            for h in (0, 1):
                for j in (0, 1):
                    self.over(h, 0, 0, j, 0)

        def out(self, turn):
            for h in (0, 1):
                for ia in (-1, 1):
                    for s in ways:
                        self.send(h, ia, 0, turn if ia < 0 else 1 - turn, "b", s, WIDE + turn)

        def near(self, turn):
            self.wait(NEAR + turn)
            if turn == 0:
                for h in (0, 1):
                    for s in ways:
                        self.send(h, -s, 0, 0 if s > 0 else 1, "a", s, FAR)
            self.out(turn)
            for h in (0, 1):
                for s in ways:
                    self.over(h, -s, 0, turn if s > 0 else 1 - turn, 1)

        def own(self, turn):
            self.wait(OWN + turn)
            if turn == 0:
                for h in (0, 1):
                    for s in ways:
                        self.send(h, 0, -s, 0 if s > 0 else 1, "b", s, BACK)
            for h in (0, 1):
                for s in ways:
                    self.over(h, 0, -s, turn if s > 0 else 1 - turn, 2)

        def out_far(self, h, turn):
            group = LATE + 1 if h == 1 and turn == 1 and self.skew else MID + turn
            for s in ways:
                self.send(h, 2, 0, turn if s > 0 else 1 - turn, "b", s, group)

        def far(self):
            self.wait(FAR)
            for turn in (0, 1):
                for h in (0, 1):
                    if h == 0 or turn == 0 or not self.skew:
                        self.out_far(h, turn)
            for h in (0, 1):
                for j in (0, 1):
                    self.over(h, 2, 0, j, 3)

        def back(self):
            self.wait(BACK)
            for h in (0, 1):
                for j in (0, 1):
                    self.over(h, 0, 2, j, 4)

        def wide(self, turn):
            self.wait(WIDE + turn, 8)
            for h in (0, 1):
                for s in ways:
                    ia = -s if turn == 0 else s
                    group = (MID + 1, LATE)[turn] if h == 1 and self.skew else LATE + turn
                    self.send(h, ia, -s, 0 if s > 0 else 1, "b", s, group)
            if turn == 1 and self.skew:
                self.out_far(1, 1)
            for h in (0, 1):
                for ia in (-1, 1):
                    for s in ways:
                        self.over(h, ia, -s, turn if ia < 0 else 1 - turn, 5)

        def crossed_far(self, h, turn, event):
            if turn == 0:
                for s in ways:
                    self.send(h, 2, -s, 0 if s > 0 else 1, "b", s, END)
            for s in ways:
                self.over(h, 2, -s, turn if s > 0 else 1 - turn, event)

        def crossed_edge(self, h, turn, event):
            for s in ways:
                self.over(h, -s if turn == 0 else s, 2, 0 if s > 0 else 1, event)

        def mid(self, turn):
            self.wait(MID + turn)
            self.crossed_far(0, turn, 6)
            if not self.skew:
                self.crossed_far(1, turn, 6)
            elif turn == 0:
                self.crossed_far(1, 0, 7)
            else:
                self.crossed_edge(1, 0, 6)

        def late(self, turn):
            self.wait(LATE + turn)
            self.crossed_edge(0, turn, 7)
            if not self.skew:
                self.crossed_edge(1, turn, 7)
            elif turn == 0:
                self.crossed_edge(1, 1, 6)
            else:
                self.crossed_far(1, 1, 7)

        def end(self):
            self.wait(END)
            for h in (0, 1):
                for j in (0, 1):
                    self.over(h, 2, 2, j, 8)

        def drain(self):
            ref = self.buf.at[0, pl.ds(0, self.buf.shape[1] - 1)]
            remote(ref, ref, sent.at[self.number], sent.at[self.number], sibling).wait_send()
            whole = self.buf.at[0]
            remote(whole, whole, side_sent.at[self.number], side_sent.at[self.number], sibling).wait_send()

    ups = Gather(0, up, False)
    downs = Gather(1, down, True)

    loads[0].wait()
    for q in range(QUARTERS):
        up[c, mine, q] = up_ref[:, q * piece:(q + 1) * piece].astype(jnp.bfloat16)
    pl.semaphore_wait(barrier, len(peers))
    ups.first()

    loads[1].wait()
    loads[2].wait()
    values = tok_ref[...].astype(jnp.float32)
    scale = lax.rsqrt(jnp.mean(values * values, axis=-1, keepdims=True) + epsilon)
    tok[x] = (values * scale * gain_ref[...]).astype(jnp.bfloat16)
    half = rows // 2

    def token_send(slot, part, s, group):
        ref = tok.at[slot, pl.ds(part * half, half)]
        remote(ref, ref, tok_send, tok_recv.at[group], at(0, 0, s)).start()

    def token_wait(group):
        ref = tok.at[0]
        remote(ref, ref, tok_send, tok_recv.at[group], sibling).wait_recv()

    for turn in (0, 1):
        for s in (1, -1):
            token_send(x, turn if s > 0 else 1 - turn, s, turn)
    loads[3].wait()
    for q in range(QUARTERS):
        down[c, mine, q] = down_ref[q * piece:(q + 1) * piece, :].astype(jnp.bfloat16)

    relative = (0, 1, -1, 2)

    def expand(places, begin, end, first_row, last_row):
        for h in (0, 1):
            numbers = [block(h, *place) for place in places]
            left = jnp.concatenate([
                jnp.concatenate(
                    [tok[ring(x, relative[r]), :, pl.ds(pl.multiple_of(f * share, share), share)] for f in numbers], axis=1
                ) for r in range(first_row, last_row)
            ], axis=0)
            span = slice(first_row * rows, last_row * rows)
            for core in (0, 1):
                slots = [core * QUARTERS + 2 * h + j for j in (0, 1)]
                right = jnp.concatenate([
                    jnp.concatenate([up[core, f, 2 * h + j] for f in numbers], axis=0) for j in (0, 1)
                ], axis=1)
                pre = jnp.dot(left, right, preferred_element_type=jnp.float32)
                for j, slot in enumerate(slots):
                    new = pre[:, j * piece:(j + 1) * piece]
                    if not begin:
                        new = new + acc[slot, span]
                    if end:
                        hidden[slot, span] = jnp.square(jnp.maximum(new, 0.0)).astype(jnp.bfloat16)
                    else:
                        acc[slot, span] = new

    groups = [
        [(0, 0), (-1, 0), (1, 0), (2, 0)], [(-1, -1), (-1, 1), (1, -1), (1, 1)], [(0, -1), (0, 1)],
        [(2, -1), (2, 1)], [(-1, 2), (1, 2)], [(0, 2), (2, 2)],
    ]

    ups.near(0)
    ups.near(1)
    ups.own(0)
    ups.own(1)
    ups.far()
    token_wait(0)
    for s in ways:
        token_send(ring(x, -s), 0 if s > 0 else 1, s, 2)
    ups.wide(0)
    token_wait(1)
    ups.wait_over(0, 1, 3)
    expand(groups[0], True, False, 0, 3)
    ups.wide(1)
    ups.back()
    ups.wait_over(5)
    expand(groups[1], False, False, 0, 3)
    ups.mid(0)
    ups.wait_over(2)
    expand(groups[2], False, False, 0, 3)
    ups.mid(1)
    downs.first()
    token_wait(2)
    expand(groups[0], True, False, 3, 4)
    expand(groups[1], False, False, 3, 4)
    expand(groups[2], False, False, 3, 4)
    ups.late(0)
    ups.late(1)
    ups.wait_over(6)
    expand(groups[3], False, False, 0, 4)
    ups.end()
    ups.wait_over(7)
    expand(groups[4], False, False, 0, 4)
    downs.near(0)
    ups.wait_over(4, 8)
    expand(groups[5], False, True, 0, 4)

    def spot(dz, dy):
        return ring(z, dz) * SIDE + ring(y, dy)

    def level_of(ref, unit, way, at_row):
        return ref[unit, way, at_row:at_row + 8].astype(jnp.float32)[0:1]

    def terms(shard, first, last):
        return acc[shard // 2, first:last, (shard % 2) * width:(shard % 2 + 1) * width]

    mid = rows // 2

    def one_copy(unit, way):
        span = pl.ds(0, len(units[unit]) * mid + 8)
        return remote(
            one_out.at[unit, way, span], one_in.at[unit, way, span], one_send.at[unit], one_recv.at[unit],
            at(0, 0, ways[way]),
        )

    def far_copy(unit):
        span = pl.ds(0, len(units[unit]) * rows + 8)
        return remote(
            one_out.at[unit, 0, span], one_in.at[unit, 0, span], one_send.at[unit], one_recv.at[unit], at(0, 0, 2)
        )

    def two_copy(unit, way):
        span = pl.ds(0, len(units[unit]) * rows + 8)
        return remote(
            two_out.at[unit, way, span], two_in.at[unit, way, span], two_send.at[unit], two_recv.at[unit],
            at(0, 0, ways[way]),
        )

    def project(first, count):
        numbers = [spot(*place) for place in shards_at[first:first + count]]
        right = jnp.concatenate([
            jnp.concatenate([down[core, f, q] for f in numbers], axis=1) for core in (0, 1) for q in range(QUARTERS)
        ], axis=0)
        parts = 1 if count > 2 else 2
        tall = 4 * rows // parts
        for part in range(parts):
            span = slice(part * tall, (part + 1) * tall)
            left = jnp.concatenate([hidden[slot, span] for slot in range(2 * QUARTERS)], axis=1)
            total = jnp.dot(left, right, preferred_element_type=jnp.float32)
            for n in range(count):
                shard = first + n
                acc[shard // 2, span, (shard % 2) * width:(shard % 2 + 1) * width] = total[:, n * width:(n + 1) * width]

    def pack(ref, unit, way, codes, level):
        tall = codes[0].shape[0]
        for n, code in enumerate(codes):
            ref[unit, way, n * tall:(n + 1) * tall] = code
        ref[unit, way, len(codes) * tall:len(codes) * tall + 8] = level

    def gather_terms(unit, first, last):
        return jnp.concatenate([terms(shard, first, last) for shard in units[unit]], axis=1)

    def launch(unit):
        if unit in direct:
            pack(one_out, unit, 0, *encode(gather_terms(unit, 3 * rows, 4 * rows)))
            far_copy(unit).start()
            for way in (0, 1):
                pack(two_out, unit, way, *encode(gather_terms(unit, (1 + way) * rows, (2 + way) * rows)))
                two_copy(unit, way).start()
        else:
            for way in (0, 1):
                first = 3 * rows + way * mid
                pack(one_out, unit, way, *encode(gather_terms(unit, first, first + mid)))
                one_copy(unit, way).start()

    def relay(unit):
        count = len(units[unit])
        ref = one_in.at[unit, :, pl.ds(0, count * mid + 8)]
        remote(ref, ref, one_send.at[unit], one_recv.at[unit], sibling).wait_recv()
        for way in (0, 1):
            level = level_of(one_in, unit, way, count * mid)
            sums = []
            for n, shard in enumerate(units[unit]):
                taken = decode(one_in[unit, way, n * mid:(n + 1) * mid], level)
                halves = [terms(shard, (1 + way) * rows + part * mid, (1 + way) * rows + (part + 1) * mid) for part in (0, 1)]
                halves[way] = halves[way] + taken
                sums.append(jnp.concatenate(halves, axis=0))
            pack(two_out, unit, way, *encode(jnp.concatenate(sums, axis=1)))
            two_copy(unit, way).start()

    def finish(unit):
        count = len(units[unit])
        ref = two_in.at[unit, :, pl.ds(0, count * rows + 8)]
        remote(ref, ref, two_send.at[unit], two_recv.at[unit], sibling).wait_recv()
        incoming = [(two_in, 0), (two_in, 1)]
        if unit in direct:
            far_copy(unit).wait_recv()
            incoming.append((one_in, 0))
        levels = [level_of(buf, unit, way, count * rows) for buf, way in incoming]
        for n, shard in enumerate(units[unit]):
            total = terms(shard, 0, rows)
            for (buf, way), level in zip(incoming, levels):
                total = total + decode(buf[unit, way, n * rows:(n + 1) * rows], level)
            f = spot(*shards_at[shard])
            out_ref[:, pl.ds(pl.multiple_of(f * width, width), width)] = total.astype(jnp.bfloat16)

    shards_at = [
        (0, 0), (-1, 0), (1, 0), (0, -1), (0, 1), (-1, -1), (-1, 1), (1, -1), (1, 1), (2, 0), (0, 2),
        (2, -1), (2, 1), (-1, 2), (1, 2), (2, 2),
    ]
    units = [(0,), (1, 2), (3, 4), (5, 6), (7, 8), (9, 10), (11, 12), (13, 14), (15,)]
    direct = (0, 1, 2)

    downs.near(1)
    downs.wait_over(0)
    project(0, 1)
    launch(0)
    downs.own(0)
    downs.own(1)
    downs.far()
    downs.wait_over(1)
    downs.wait_over(2)
    project(1, 4)
    launch(1)
    launch(2)
    downs.wide(0)
    downs.wait_over(3)
    downs.wide(1)
    finish(0)
    downs.wait_over(5)
    project(5, 4)
    launch(3)
    launch(4)
    downs.back()
    downs.mid(0)
    downs.wait_over(4)
    project(9, 2)
    launch(5)
    downs.mid(1)
    downs.late(0)
    relay(3)
    downs.wait_over(6)
    project(11, 2)
    launch(6)
    relay(4)
    downs.late(1)
    finish(1)
    finish(2)
    downs.end()
    downs.wait_over(7)
    project(13, 2)
    launch(7)
    downs.wait_over(8)
    project(15, 1)
    launch(8)
    relay(5)
    relay(6)
    relay(7)
    relay(8)
    finish(3)
    finish(4)
    finish(5)
    finish(6)
    finish(7)
    finish(8)

    ref = tok.at[pl.ds(0, 3)]
    remote(ref, ref, tok_send, tok_send, sibling).wait_send()
    for unit in range(len(units)):
        for way in (0, 1):
            two_copy(unit, way).wait_send()
            if unit not in direct:
                one_copy(unit, way).wait_send()
        if unit in direct:
            far_copy(unit).wait_send()
    ups.drain()
    downs.drain()


def solution(mesh):
    fs, tp = mesh.shape["fs"], mesh.shape["tp"]
    placed = (P(("fs", "tp"), None), P(), P("fs", "tp"), P("tp", "fs"))

    def whole(tokens, norm_gain, up_weight, down_weight):
        rows, depth = tokens.shape
        share, span = up_weight.shape
        width = down_weight.shape[1]
        piece = span // QUARTERS
        groups = tp // 2
        vm, dma = pltpu.VMEM, pltpu.SemaphoreType.DMA
        low, full = jnp.bfloat16, jnp.float32
        return pl.pallas_call(
            kernel,
            out_shape=jax.ShapeDtypeStruct((rows, depth), low),
            in_specs=[pl.BlockSpec(memory_space=pltpu.HBM)] * 4,
            out_specs=pl.BlockSpec(memory_space=pltpu.VMEM),
            scratch_shapes=[
                vm((rows, depth), low),
                vm((1, depth), full),
                vm((share, span), full),
                vm((span, width), full),
                vm((groups, rows, depth), low),
                vm((2, fs, QUARTERS, share, piece), low),
                vm((2, fs, QUARTERS, piece, width), low),
                vm((2 * QUARTERS, groups * rows, piece), full),
                vm((2 * QUARTERS, groups * rows, piece), low),
                vm((UNITS, 2, 2 * rows + 8, LANES), low),
                vm((UNITS, 2, 2 * rows + 8, LANES), low),
                vm((UNITS, 2, 2 * rows + 8, LANES), low),
                vm((UNITS, 2, 2 * rows + 8, LANES), low),
                dma((4,)), dma, dma((3,)),
                dma((2, 13)), dma((2, 9)), dma((2,)), dma((2,)), dma((UNITS,)), dma((UNITS,)), dma((UNITS,)), dma((UNITS,)),
            ],
            compiler_params=pltpu.CompilerParams(
                collective_id=0, has_side_effects=True, vmem_limit_bytes=VMEM_LIMIT
            ),
        )(*(
            pltpu.with_memory_space_constraint(array, pltpu.HBM)
            for array in (tokens, norm_gain.reshape(1, depth), up_weight, down_weight)
        ))

    return jax.shard_map(
        whole, mesh=mesh, in_specs=placed, out_specs=P(("fs", "tp"), None), check_vma=False
    )
```

```python
import functools

import jax
import jax.numpy as jnp
from jax import lax
from jax.experimental import pallas as pl
from jax.experimental.pallas import tpu as pltpu
from jax.sharding import PartitionSpec as P

epsilon = 1e-06
MESH = pl.DeviceIdType.MESH
VMEM_LIMIT = 48_000_000
SIDE = 4
QUARTERS = 4
LANES = 128
UNITS = 9
POWER = 9
PEAK = 11585.0
TINY = 1e-30


def encode(block):
    largest = jnp.max(jnp.abs(block), axis=0, keepdims=True)
    level = largest[:, :LANES]
    for start in range(LANES, block.shape[1], LANES):
        level = jnp.maximum(level, largest[:, start:start + LANES])
    level = jnp.maximum(level, TINY).astype(jnp.bfloat16)
    factor = PEAK / level.astype(jnp.float32)
    codes = []
    for start in range(0, block.shape[1], LANES):
        t = block[:, start:start + LANES] * factor
        t2 = t * t
        t4 = t2 * t2
        codes.append((t4 * t4 * t).astype(jnp.bfloat16))
    return codes, jnp.broadcast_to(level, (8, LANES))


def decode(code, level):
    y = code.astype(jnp.float32)
    size = jnp.exp(jnp.log(jnp.maximum(jnp.abs(y), 1e-38)) * (1.0 / POWER)) * (level * (1.0 / PEAK))
    return jnp.where(y > 0.0, size, jnp.where(y < 0.0, -size, 0.0))


def kernel(
    tok_hbm, gain_hbm, up_hbm, down_hbm, out_ref,
    tok_ref, gain_ref, up_ref, down_ref, tok, up, down, acc, hidden, one_out, one_in, two_out, two_in,
    load, tok_send, tok_recv, arrived, crossed, sent, side_sent, one_send, one_recv, two_send, two_recv,
):
    fs, tp = lax.axis_index("fs"), lax.axis_index("tp")
    z, y = fs // SIDE, lax.rem(fs, SIDE)
    x, c = tp // 2, lax.rem(tp, 2)
    other = 1 - c
    mine = fs
    rows = tok.shape[1]
    share = up.shape[3]
    piece = up.shape[4]
    width = down.shape[4]

    def ring(place, step):
        return lax.rem(place + (step + SIDE), SIDE)

    def at(dz, dy, dx):
        return (ring(z, dz) * SIDE + ring(y, dy), ring(x, dx) * 2 + c)

    sibling = (fs, x * 2 + other)

    def remote(src, dst, send, recv, to):
        return pltpu.make_async_remote_copy(
            src_ref=src, dst_ref=dst, send_sem=send, recv_sem=recv, device_id=to, device_id_type=MESH
        )

    barrier = pltpu.get_barrier_semaphore()
    peers = [at(1, 0, 0), at(-1, 0, 0), at(0, 1, 0), at(0, -1, 0), at(0, 0, 1), at(0, 0, -1), at(0, 0, 2), sibling]
    for to in peers:
        pl.semaphore_signal(barrier, inc=1, device_id=to, device_id_type=MESH)

    loads = [
        pltpu.make_async_copy(src, dst, load.at[n])
        for n, (src, dst) in enumerate([(up_hbm, up_ref), (tok_hbm, tok_ref), (gain_hbm, gain_ref), (down_hbm, down_ref)])
    ]
    loads[0].start()

    def block(h, ia, ib):
        dz, dy = (ia, ib) if h == 0 else (ib, ia)
        return ring(z, dz) * SIDE + ring(y, dy)

    ways = (1, -1)
    NEAR, OWN, FAR, BACK, WIDE, MID, LATE, END = 0, 2, 4, 5, 6, 8, 10, 12

    class Gather:
        def __init__(self, number, buf, skew):
            self.number, self.buf, self.skew = number, buf, skew

        def send(self, h, ia, ib, j, axis, s, group):
            along_z = (axis == "a") == (h == 0)
            to = at(s, 0, 0) if along_z else at(0, s, 0)
            ref = self.buf.at[c, block(h, ia, ib), 2 * h + j]
            remote(ref, ref, sent.at[self.number], arrived.at[self.number, group], to).start()

        def wait(self, group, count=4):
            ref = self.buf.at[c, pl.ds(0, count), 0]
            remote(ref, ref, sent.at[self.number], arrived.at[self.number, group], sibling).wait_recv()

        def over(self, h, ia, ib, j, event):
            ref = self.buf.at[c, block(h, ia, ib), 2 * h + j]
            remote(ref, ref, side_sent.at[self.number], crossed.at[self.number, event], sibling).start()

        def wait_over(self, *events):
            for event in events:
                ref = self.buf.at[other, pl.ds(0, (2, 4, 4, 2, 2, 8, 4, 4, 2)[event]), pl.ds(0, 2)]
                remote(ref, ref, side_sent.at[self.number], crossed.at[self.number, event], sibling).wait_recv()

        def first(self):
            for axis, group in (("a", NEAR), ("b", OWN)):
                for turn in (0, 1):
                    for h in (0, 1):
                        for s in ways:
                            self.send(h, 0, 0, turn if s > 0 else 1 - turn, axis, s, group + turn)
            for h in (0, 1):
                for j in (0, 1):
                    self.over(h, 0, 0, j, 0)

        def out(self, turn):
            for h in (0, 1):
                for ia in (-1, 1):
                    for s in ways:
                        self.send(h, ia, 0, turn if ia < 0 else 1 - turn, "b", s, WIDE + turn)

        def near(self, turn):
            self.wait(NEAR + turn)
            if turn == 0:
                for h in (0, 1):
                    for s in ways:
                        self.send(h, -s, 0, 0 if s > 0 else 1, "a", s, FAR)
            self.out(turn)
            for h in (0, 1):
                for s in ways:
                    self.over(h, -s, 0, turn if s > 0 else 1 - turn, 1)

        def own(self, turn):
            self.wait(OWN + turn)
            if turn == 0:
                for h in (0, 1):
                    for s in ways:
                        self.send(h, 0, -s, 0 if s > 0 else 1, "b", s, BACK)
            for h in (0, 1):
                for s in ways:
                    self.over(h, 0, -s, turn if s > 0 else 1 - turn, 2)

        def out_far(self, h, turn):
            group = LATE + 1 if h == 1 and turn == 1 and self.skew else MID + turn
            for s in ways:
                self.send(h, 2, 0, turn if s > 0 else 1 - turn, "b", s, group)

        def far(self):
            self.wait(FAR)
            for turn in (0, 1):
                for h in (0, 1):
                    if h == 0 or turn == 0 or not self.skew:
                        self.out_far(h, turn)
            for h in (0, 1):
                for j in (0, 1):
                    self.over(h, 2, 0, j, 3)

        def back(self):
            self.wait(BACK)
            for h in (0, 1):
                for j in (0, 1):
                    self.over(h, 0, 2, j, 4)

        def wide(self, turn):
            self.wait(WIDE + turn, 8)
            for h in (0, 1):
                for s in ways:
                    ia = -s if turn == 0 else s
                    group = (MID + 1, LATE)[turn] if h == 1 and self.skew else LATE + turn
                    self.send(h, ia, -s, 0 if s > 0 else 1, "b", s, group)
            if turn == 1 and self.skew:
                self.out_far(1, 1)
            for h in (0, 1):
                for ia in (-1, 1):
                    for s in ways:
                        self.over(h, ia, -s, turn if ia < 0 else 1 - turn, 5)

        def crossed_far(self, h, turn, event):
            if turn == 0:
                for s in ways:
                    self.send(h, 2, -s, 0 if s > 0 else 1, "b", s, END)
            for s in ways:
                self.over(h, 2, -s, turn if s > 0 else 1 - turn, event)

        def crossed_edge(self, h, turn, event):
            for s in ways:
                self.over(h, -s if turn == 0 else s, 2, 0 if s > 0 else 1, event)

        def mid(self, turn):
            self.wait(MID + turn)
            self.crossed_far(0, turn, 6)
            if not self.skew:
                self.crossed_far(1, turn, 6)
            elif turn == 0:
                self.crossed_far(1, 0, 7)
            else:
                self.crossed_edge(1, 0, 6)

        def late(self, turn):
            self.wait(LATE + turn)
            self.crossed_edge(0, turn, 7)
            if not self.skew:
                self.crossed_edge(1, turn, 7)
            elif turn == 0:
                self.crossed_edge(1, 1, 6)
            else:
                self.crossed_far(1, 1, 7)

        def end(self):
            self.wait(END)
            for h in (0, 1):
                for j in (0, 1):
                    self.over(h, 2, 2, j, 8)

        def drain(self):
            ref = self.buf.at[0, pl.ds(0, self.buf.shape[1] - 1)]
            remote(ref, ref, sent.at[self.number], sent.at[self.number], sibling).wait_send()
            whole = self.buf.at[0]
            remote(whole, whole, side_sent.at[self.number], side_sent.at[self.number], sibling).wait_send()

    ups = Gather(0, up, False)
    downs = Gather(1, down, True)

    loads[0].wait()
    for copy in loads[1:]:
        copy.start()
    for q in range(QUARTERS):
        up[c, mine, q] = up_ref[:, q * piece:(q + 1) * piece].astype(jnp.bfloat16)
    pl.semaphore_wait(barrier, len(peers))
    ups.first()

    loads[1].wait()
    loads[2].wait()
    values = tok_ref[...].astype(jnp.float32)
    scale = lax.rsqrt(jnp.mean(values * values, axis=-1, keepdims=True) + epsilon)
    tok[x] = (values * scale * gain_ref[...]).astype(jnp.bfloat16)
    half = rows // 2

    def token_send(slot, part, s, group):
        ref = tok.at[slot, pl.ds(part * half, half)]
        remote(ref, ref, tok_send, tok_recv.at[group], at(0, 0, s)).start()

    def token_wait(group):
        ref = tok.at[0]
        remote(ref, ref, tok_send, tok_recv.at[group], sibling).wait_recv()

    for turn in (0, 1):
        for s in (1, -1):
            token_send(x, turn if s > 0 else 1 - turn, s, turn)
    loads[3].wait()
    for q in range(QUARTERS):
        down[c, mine, q] = down_ref[q * piece:(q + 1) * piece, :].astype(jnp.bfloat16)

    relative = (0, 1, -1, 2)

    def expand(places, begin, end, first_row, last_row):
        for h in (0, 1):
            numbers = [block(h, *place) for place in places]
            left = jnp.concatenate([
                jnp.concatenate(
                    [tok[ring(x, relative[r]), :, pl.ds(pl.multiple_of(f * share, share), share)] for f in numbers], axis=1
                ) for r in range(first_row, last_row)
            ], axis=0)
            span = slice(first_row * rows, last_row * rows)
            for core in (0, 1):
                slots = [core * QUARTERS + 2 * h + j for j in (0, 1)]
                right = jnp.concatenate([
                    jnp.concatenate([up[core, f, 2 * h + j] for f in numbers], axis=0) for j in (0, 1)
                ], axis=1)
                pre = jnp.dot(left, right, preferred_element_type=jnp.float32)
                for j, slot in enumerate(slots):
                    new = pre[:, j * piece:(j + 1) * piece]
                    if not begin:
                        new = new + acc[slot, span]
                    if end:
                        hidden[slot, span] = jnp.square(jnp.maximum(new, 0.0)).astype(jnp.bfloat16)
                    else:
                        acc[slot, span] = new

    groups = [
        [(0, 0), (-1, 0), (1, 0), (2, 0)], [(-1, -1), (-1, 1), (1, -1), (1, 1)], [(0, -1), (0, 1)],
        [(2, -1), (2, 1)], [(-1, 2), (1, 2)], [(0, 2), (2, 2)],
    ]

    ups.near(0)
    ups.near(1)
    ups.own(0)
    ups.own(1)
    ups.far()
    token_wait(0)
    for s in ways:
        token_send(ring(x, -s), 0 if s > 0 else 1, s, 2)
    ups.wide(0)
    token_wait(1)
    ups.wait_over(0, 1, 3)
    expand(groups[0], True, False, 0, 3)
    ups.wide(1)
    ups.back()
    ups.wait_over(5)
    expand(groups[1], False, False, 0, 3)
    ups.mid(0)
    ups.wait_over(2)
    expand(groups[2], False, False, 0, 3)
    ups.mid(1)
    downs.first()
    token_wait(2)
    expand(groups[0], True, False, 3, 4)
    expand(groups[1], False, False, 3, 4)
    expand(groups[2], False, False, 3, 4)
    ups.late(0)
    ups.late(1)
    ups.wait_over(6)
    expand(groups[3], False, False, 0, 4)
    ups.end()
    ups.wait_over(7)
    expand(groups[4], False, False, 0, 4)
    downs.near(0)
    ups.wait_over(4, 8)
    expand(groups[5], False, True, 0, 4)

    def spot(dz, dy):
        return ring(z, dz) * SIDE + ring(y, dy)

    def level_of(ref, unit, way, at_row):
        return ref[unit, way, at_row:at_row + 8].astype(jnp.float32)[0:1]

    def terms(shard, first, last):
        return acc[shard // 2, first:last, (shard % 2) * width:(shard % 2 + 1) * width]

    mid = rows // 2

    def one_copy(unit, way):
        span = pl.ds(0, len(units[unit]) * mid + 8)
        return remote(
            one_out.at[unit, way, span], one_in.at[unit, way, span], one_send.at[unit], one_recv.at[unit],
            at(0, 0, ways[way]),
        )

    def far_copy(unit):
        span = pl.ds(0, len(units[unit]) * rows + 8)
        return remote(
            one_out.at[unit, 0, span], one_in.at[unit, 0, span], one_send.at[unit], one_recv.at[unit], at(0, 0, 2)
        )

    def two_copy(unit, way):
        span = pl.ds(0, len(units[unit]) * rows + 8)
        return remote(
            two_out.at[unit, way, span], two_in.at[unit, way, span], two_send.at[unit], two_recv.at[unit],
            at(0, 0, ways[way]),
        )

    def project(first, count):
        numbers = [spot(*place) for place in shards_at[first:first + count]]
        right = jnp.concatenate([
            jnp.concatenate([down[core, f, q] for f in numbers], axis=1) for core in (0, 1) for q in range(QUARTERS)
        ], axis=0)
        parts = 1 if count > 2 else 2
        tall = 4 * rows // parts
        for part in range(parts):
            span = slice(part * tall, (part + 1) * tall)
            left = jnp.concatenate([hidden[slot, span] for slot in range(2 * QUARTERS)], axis=1)
            total = jnp.dot(left, right, preferred_element_type=jnp.float32)
            for n in range(count):
                shard = first + n
                acc[shard // 2, span, (shard % 2) * width:(shard % 2 + 1) * width] = total[:, n * width:(n + 1) * width]

    def pack(ref, unit, way, codes, level):
        tall = codes[0].shape[0]
        for n, code in enumerate(codes):
            ref[unit, way, n * tall:(n + 1) * tall] = code
        ref[unit, way, len(codes) * tall:len(codes) * tall + 8] = level

    def gather_terms(unit, first, last):
        return jnp.concatenate([terms(shard, first, last) for shard in units[unit]], axis=1)

    def launch(unit):
        if unit in direct:
            pack(one_out, unit, 0, *encode(gather_terms(unit, 3 * rows, 4 * rows)))
            far_copy(unit).start()
            for way in (0, 1):
                pack(two_out, unit, way, *encode(gather_terms(unit, (1 + way) * rows, (2 + way) * rows)))
                two_copy(unit, way).start()
        else:
            for way in (0, 1):
                first = 3 * rows + way * mid
                pack(one_out, unit, way, *encode(gather_terms(unit, first, first + mid)))
                one_copy(unit, way).start()

    def relay(unit):
        count = len(units[unit])
        ref = one_in.at[unit, :, pl.ds(0, count * mid + 8)]
        remote(ref, ref, one_send.at[unit], one_recv.at[unit], sibling).wait_recv()
        for way in (0, 1):
            level = level_of(one_in, unit, way, count * mid)
            sums = []
            for n, shard in enumerate(units[unit]):
                taken = decode(one_in[unit, way, n * mid:(n + 1) * mid], level)
                halves = [terms(shard, (1 + way) * rows + part * mid, (1 + way) * rows + (part + 1) * mid) for part in (0, 1)]
                halves[way] = halves[way] + taken
                sums.append(jnp.concatenate(halves, axis=0))
            pack(two_out, unit, way, *encode(jnp.concatenate(sums, axis=1)))
            two_copy(unit, way).start()

    def finish(unit):
        count = len(units[unit])
        ref = two_in.at[unit, :, pl.ds(0, count * rows + 8)]
        remote(ref, ref, two_send.at[unit], two_recv.at[unit], sibling).wait_recv()
        incoming = [(two_in, 0), (two_in, 1)]
        if unit in direct:
            far_copy(unit).wait_recv()
            incoming.append((one_in, 0))
        levels = [level_of(buf, unit, way, count * rows) for buf, way in incoming]
        for n, shard in enumerate(units[unit]):
            total = terms(shard, 0, rows)
            for (buf, way), level in zip(incoming, levels):
                total = total + decode(buf[unit, way, n * rows:(n + 1) * rows], level)
            f = spot(*shards_at[shard])
            out_ref[:, pl.ds(pl.multiple_of(f * width, width), width)] = total.astype(jnp.bfloat16)

    shards_at = [
        (0, 0), (-1, 0), (1, 0), (0, -1), (0, 1), (-1, -1), (-1, 1), (1, -1), (1, 1), (2, 0), (0, 2),
        (2, -1), (2, 1), (-1, 2), (1, 2), (2, 2),
    ]
    units = [(0,), (1, 2), (3, 4), (5, 6), (7, 8), (9, 10), (11, 12), (13, 14), (15,)]
    direct = (0, 1, 2, 5)

    downs.near(1)
    downs.wait_over(0)
    project(0, 1)
    launch(0)
    downs.own(0)
    downs.own(1)
    downs.far()
    downs.wait_over(1)
    downs.wait_over(2)
    project(1, 4)
    launch(1)
    launch(2)
    downs.wide(0)
    downs.wait_over(3)
    downs.wide(1)
    finish(0)
    downs.wait_over(5)
    project(5, 4)
    launch(3)
    launch(4)
    downs.back()
    downs.mid(0)
    downs.wait_over(4)
    project(9, 2)
    launch(5)
    downs.mid(1)
    downs.late(0)
    relay(3)
    downs.wait_over(6)
    project(11, 2)
    launch(6)
    relay(4)
    downs.late(1)
    finish(1)
    finish(2)
    downs.end()
    downs.wait_over(7)
    project(13, 2)
    launch(7)
    downs.wait_over(8)
    project(15, 1)
    launch(8)
    relay(6)
    relay(7)
    relay(8)
    finish(3)
    finish(4)
    finish(5)
    finish(6)
    finish(7)
    finish(8)

    ref = tok.at[pl.ds(0, 3)]
    remote(ref, ref, tok_send, tok_send, sibling).wait_send()
    for unit in range(len(units)):
        for way in (0, 1):
            two_copy(unit, way).wait_send()
            if unit not in direct:
                one_copy(unit, way).wait_send()
        if unit in direct:
            far_copy(unit).wait_send()
    ups.drain()
    downs.drain()


def solution(mesh):
    fs, tp = mesh.shape["fs"], mesh.shape["tp"]
    placed = (P(("fs", "tp"), None), P(), P("fs", "tp"), P("tp", "fs"))

    def whole(tokens, norm_gain, up_weight, down_weight):
        rows, depth = tokens.shape
        share, span = up_weight.shape
        width = down_weight.shape[1]
        piece = span // QUARTERS
        groups = tp // 2
        vm, dma = pltpu.VMEM, pltpu.SemaphoreType.DMA
        low, full = jnp.bfloat16, jnp.float32
        return pl.pallas_call(
            kernel,
            out_shape=jax.ShapeDtypeStruct((rows, depth), low),
            in_specs=[pl.BlockSpec(memory_space=pltpu.HBM)] * 4,
            out_specs=pl.BlockSpec(memory_space=pltpu.VMEM),
            scratch_shapes=[
                vm((rows, depth), low),
                vm((1, depth), full),
                vm((share, span), full),
                vm((span, width), full),
                vm((groups, rows, depth), low),
                vm((2, fs, QUARTERS, share, piece), low),
                vm((2, fs, QUARTERS, piece, width), low),
                vm((2 * QUARTERS, groups * rows, piece), full),
                vm((2 * QUARTERS, groups * rows, piece), low),
                vm((UNITS, 2, 2 * rows + 8, LANES), low),
                vm((UNITS, 2, 2 * rows + 8, LANES), low),
                vm((UNITS, 2, 2 * rows + 8, LANES), low),
                vm((UNITS, 2, 2 * rows + 8, LANES), low),
                dma((4,)), dma, dma((3,)),
                dma((2, 13)), dma((2, 9)), dma((2,)), dma((2,)), dma((UNITS,)), dma((UNITS,)), dma((UNITS,)), dma((UNITS,)),
            ],
            compiler_params=pltpu.CompilerParams(
                collective_id=0, has_side_effects=True, vmem_limit_bytes=VMEM_LIMIT
            ),
        )(*(
            pltpu.with_memory_space_constraint(array, pltpu.HBM)
            for array in (tokens, norm_gain.reshape(1, depth), up_weight, down_weight)
        ))

    return jax.shard_map(
        whole, mesh=mesh, in_specs=placed, out_specs=P(("fs", "tp"), None), check_vma=False
    )
```

```python
import functools

import jax
import jax.numpy as jnp
from jax import lax
from jax.experimental import pallas as pl
from jax.experimental.pallas import tpu as pltpu
from jax.sharding import PartitionSpec as P

epsilon = 1e-06
MESH = pl.DeviceIdType.MESH
VMEM_LIMIT = 48_000_000
SIDE = 4
QUARTERS = 4
LANES = 128
UNITS = 9
POWER = 9
PEAK = 11585.0
TINY = 1e-30


def encode(block):
    largest = jnp.max(jnp.abs(block), axis=0, keepdims=True)
    level = largest[:, :LANES]
    for start in range(LANES, block.shape[1], LANES):
        level = jnp.maximum(level, largest[:, start:start + LANES])
    level = jnp.maximum(level, TINY).astype(jnp.bfloat16)
    factor = PEAK / level.astype(jnp.float32)
    codes = []
    for start in range(0, block.shape[1], LANES):
        t = block[:, start:start + LANES] * factor
        t2 = t * t
        t4 = t2 * t2
        codes.append((t4 * t4 * t).astype(jnp.bfloat16))
    return codes, jnp.broadcast_to(level, (8, LANES))


def decode(code, level):
    y = code.astype(jnp.float32)
    size = jnp.exp(jnp.log(jnp.maximum(jnp.abs(y), 1e-38)) * (1.0 / POWER)) * (level * (1.0 / PEAK))
    return jnp.where(y > 0.0, size, jnp.where(y < 0.0, -size, 0.0))


def kernel(
    tok_hbm, gain_hbm, up_hbm, down_hbm, out_ref,
    tok_ref, gain_ref, up_ref, down_ref, tok, up, down, acc, hidden, one_out, one_in, two_out, two_in,
    load, tok_send, tok_recv, arrived, crossed, sent, side_sent, one_send, one_recv, two_send, two_recv,
):
    fs, tp = lax.axis_index("fs"), lax.axis_index("tp")
    z, y = fs // SIDE, lax.rem(fs, SIDE)
    x, c = tp // 2, lax.rem(tp, 2)
    other = 1 - c
    mine = fs
    rows = tok.shape[1]
    share = up.shape[3]
    piece = up.shape[4]
    width = down.shape[4]

    def ring(place, step):
        return lax.rem(place + (step + SIDE), SIDE)

    def at(dz, dy, dx):
        return (ring(z, dz) * SIDE + ring(y, dy), ring(x, dx) * 2 + c)

    sibling = (fs, x * 2 + other)

    def remote(src, dst, send, recv, to):
        return pltpu.make_async_remote_copy(
            src_ref=src, dst_ref=dst, send_sem=send, recv_sem=recv, device_id=to, device_id_type=MESH
        )

    barrier = pltpu.get_barrier_semaphore()
    peers = [at(1, 0, 0), at(-1, 0, 0), at(0, 1, 0), at(0, -1, 0), at(0, 0, 1), at(0, 0, -1), sibling]
    for to in peers:
        pl.semaphore_signal(barrier, inc=1, device_id=to, device_id_type=MESH)

    loads = [
        pltpu.make_async_copy(src, dst, load.at[n])
        for n, (src, dst) in enumerate([(up_hbm, up_ref), (tok_hbm, tok_ref), (gain_hbm, gain_ref), (down_hbm, down_ref)])
    ]
    loads[0].start()

    def block(h, ia, ib):
        dz, dy = (ia, ib) if h == 0 else (ib, ia)
        return ring(z, dz) * SIDE + ring(y, dy)

    ways = (1, -1)
    NEAR, OWN, FAR, BACK, WIDE, MID, LATE, END = 0, 2, 4, 5, 6, 8, 10, 12

    class Gather:
        def __init__(self, number, buf, skew):
            self.number, self.buf, self.skew = number, buf, skew

        def send(self, h, ia, ib, j, axis, s, group):
            along_z = (axis == "a") == (h == 0)
            to = at(s, 0, 0) if along_z else at(0, s, 0)
            ref = self.buf.at[c, block(h, ia, ib), 2 * h + j]
            remote(ref, ref, sent.at[self.number], arrived.at[self.number, group], to).start()

        def wait(self, group, count=4):
            ref = self.buf.at[c, pl.ds(0, count), 0]
            remote(ref, ref, sent.at[self.number], arrived.at[self.number, group], sibling).wait_recv()

        def over(self, h, ia, ib, j, event):
            ref = self.buf.at[c, block(h, ia, ib), 2 * h + j]
            remote(ref, ref, side_sent.at[self.number], crossed.at[self.number, event], sibling).start()

        def wait_over(self, *events):
            for event in events:
                ref = self.buf.at[other, pl.ds(0, (2, 4, 4, 2, 2, 8, 4, 4, 2)[event]), pl.ds(0, 2)]
                remote(ref, ref, side_sent.at[self.number], crossed.at[self.number, event], sibling).wait_recv()

        def first(self):
            for axis, group in (("a", NEAR), ("b", OWN)):
                for turn in (0, 1):
                    for h in (0, 1):
                        for s in ways:
                            self.send(h, 0, 0, turn if s > 0 else 1 - turn, axis, s, group + turn)
            for h in (0, 1):
                for j in (0, 1):
                    self.over(h, 0, 0, j, 0)

        def out(self, turn):
            for h in (0, 1):
                for ia in (-1, 1):
                    for s in ways:
                        self.send(h, ia, 0, turn if ia < 0 else 1 - turn, "b", s, WIDE + turn)

        def near(self, turn):
            self.wait(NEAR + turn)
            if turn == 0:
                for h in (0, 1):
                    for s in ways:
                        self.send(h, -s, 0, 0 if s > 0 else 1, "a", s, FAR)
            self.out(turn)
            for h in (0, 1):
                for s in ways:
                    self.over(h, -s, 0, turn if s > 0 else 1 - turn, 1)

        def own(self, turn):
            self.wait(OWN + turn)
            if turn == 0:
                for h in (0, 1):
                    for s in ways:
                        self.send(h, 0, -s, 0 if s > 0 else 1, "b", s, BACK)
            for h in (0, 1):
                for s in ways:
                    self.over(h, 0, -s, turn if s > 0 else 1 - turn, 2)

        def out_far(self, h, turn):
            group = LATE + 1 if h == 1 and turn == 1 and self.skew else MID + turn
            for s in ways:
                self.send(h, 2, 0, turn if s > 0 else 1 - turn, "b", s, group)

        def far(self):
            self.wait(FAR)
            for turn in (0, 1):
                for h in (0, 1):
                    if h == 0 or turn == 0 or not self.skew:
                        self.out_far(h, turn)
            for h in (0, 1):
                for j in (0, 1):
                    self.over(h, 2, 0, j, 3)

        def back(self):
            self.wait(BACK)
            for h in (0, 1):
                for j in (0, 1):
                    self.over(h, 0, 2, j, 4)

        def wide(self, turn):
            self.wait(WIDE + turn, 8)
            for h in (0, 1):
                for s in ways:
                    ia = -s if turn == 0 else s
                    group = (MID + 1, LATE)[turn] if h == 1 and self.skew else LATE + turn
                    self.send(h, ia, -s, 0 if s > 0 else 1, "b", s, group)
            if turn == 1 and self.skew:
                self.out_far(1, 1)
            for h in (0, 1):
                for ia in (-1, 1):
                    for s in ways:
                        self.over(h, ia, -s, turn if ia < 0 else 1 - turn, 5)

        def crossed_far(self, h, turn, event):
            if turn == 0:
                for s in ways:
                    self.send(h, 2, -s, 0 if s > 0 else 1, "b", s, END)
            for s in ways:
                self.over(h, 2, -s, turn if s > 0 else 1 - turn, event)

        def crossed_edge(self, h, turn, event):
            for s in ways:
                self.over(h, -s if turn == 0 else s, 2, 0 if s > 0 else 1, event)

        def mid(self, turn):
            self.wait(MID + turn)
            self.crossed_far(0, turn, 6)
            if not self.skew:
                self.crossed_far(1, turn, 6)
            elif turn == 0:
                self.crossed_far(1, 0, 7)
            else:
                self.crossed_edge(1, 0, 6)

        def late(self, turn):
            self.wait(LATE + turn)
            self.crossed_edge(0, turn, 7)
            if not self.skew:
                self.crossed_edge(1, turn, 7)
            elif turn == 0:
                self.crossed_edge(1, 1, 6)
            else:
                self.crossed_far(1, 1, 7)

        def end(self):
            self.wait(END)
            for h in (0, 1):
                for j in (0, 1):
                    self.over(h, 2, 2, j, 8)

        def drain(self):
            ref = self.buf.at[0, pl.ds(0, self.buf.shape[1] - 1)]
            remote(ref, ref, sent.at[self.number], sent.at[self.number], sibling).wait_send()
            whole = self.buf.at[0]
            remote(whole, whole, side_sent.at[self.number], side_sent.at[self.number], sibling).wait_send()

    ups = Gather(0, up, False)
    downs = Gather(1, down, True)

    loads[0].wait()
    for copy in loads[1:]:
        copy.start()
    for q in range(QUARTERS):
        up[c, mine, q] = up_ref[:, q * piece:(q + 1) * piece].astype(jnp.bfloat16)
    pl.semaphore_wait(barrier, len(peers))
    ups.first()

    loads[1].wait()
    loads[2].wait()
    values = tok_ref[...].astype(jnp.float32)
    scale = lax.rsqrt(jnp.mean(values * values, axis=-1, keepdims=True) + epsilon)
    tok[x] = (values * scale * gain_ref[...]).astype(jnp.bfloat16)
    half = rows // 2

    def token_send(slot, part, s, group):
        ref = tok.at[slot, pl.ds(part * half, half)]
        remote(ref, ref, tok_send, tok_recv.at[group], at(0, 0, s)).start()

    def token_wait(group):
        ref = tok.at[0]
        remote(ref, ref, tok_send, tok_recv.at[group], sibling).wait_recv()

    for turn in (0, 1):
        for s in (1, -1):
            token_send(x, turn if s > 0 else 1 - turn, s, turn)
    loads[3].wait()
    for q in range(QUARTERS):
        down[c, mine, q] = down_ref[q * piece:(q + 1) * piece, :].astype(jnp.bfloat16)

    relative = (0, 1, -1, 2)

    def expand(places, begin, end, first_row, last_row):
        for h in (0, 1):
            numbers = [block(h, *place) for place in places]
            left = jnp.concatenate([
                jnp.concatenate(
                    [tok[ring(x, relative[r]), :, pl.ds(pl.multiple_of(f * share, share), share)] for f in numbers], axis=1
                ) for r in range(first_row, last_row)
            ], axis=0)
            span = slice(first_row * rows, last_row * rows)
            for core in (0, 1):
                slots = [core * QUARTERS + 2 * h + j for j in (0, 1)]
                right = jnp.concatenate([
                    jnp.concatenate([up[core, f, 2 * h + j] for f in numbers], axis=0) for j in (0, 1)
                ], axis=1)
                pre = jnp.dot(left, right, preferred_element_type=jnp.float32)
                for j, slot in enumerate(slots):
                    new = pre[:, j * piece:(j + 1) * piece]
                    if not begin:
                        new = new + acc[slot, span]
                    if end:
                        hidden[slot, span] = jnp.square(jnp.maximum(new, 0.0)).astype(jnp.bfloat16)
                    else:
                        acc[slot, span] = new

    groups = [
        [(0, 0), (-1, 0), (1, 0), (2, 0)], [(-1, -1), (-1, 1), (1, -1), (1, 1)], [(0, -1), (0, 1)],
        [(2, -1), (2, 1)], [(-1, 2), (1, 2)], [(0, 2), (2, 2)],
    ]

    ups.near(0)
    ups.near(1)
    ups.own(0)
    ups.own(1)
    ups.far()
    token_wait(0)
    for s in ways:
        token_send(ring(x, -s), 0 if s > 0 else 1, s, 2)
    ups.wide(0)
    token_wait(1)
    ups.wait_over(0, 1, 3)
    expand(groups[0], True, False, 0, 3)
    ups.wide(1)
    ups.back()
    ups.wait_over(5)
    expand(groups[1], False, False, 0, 3)
    ups.mid(0)
    ups.wait_over(2)
    expand(groups[2], False, False, 0, 3)
    ups.mid(1)
    downs.first()
    token_wait(2)
    expand(groups[0], True, False, 3, 4)
    expand(groups[1], False, False, 3, 4)
    expand(groups[2], False, False, 3, 4)
    ups.late(0)
    ups.late(1)
    ups.wait_over(6)
    expand(groups[3], False, False, 0, 4)
    ups.end()
    ups.wait_over(7)
    expand(groups[4], False, False, 0, 4)
    downs.near(0)
    ups.wait_over(4, 8)
    expand(groups[5], False, True, 0, 4)

    def spot(dz, dy):
        return ring(z, dz) * SIDE + ring(y, dy)

    def level_of(ref, unit, way, at_row):
        return ref[unit, way, at_row:at_row + 8].astype(jnp.float32)[0:1]

    def terms(shard, first, last):
        return acc[shard // 2, first:last, (shard % 2) * width:(shard % 2 + 1) * width]

    mid = rows // 2

    def one_copy(unit, way):
        span = pl.ds(0, len(units[unit]) * mid + 8)
        return remote(
            one_out.at[unit, way, span], one_in.at[unit, way, span], one_send.at[unit], one_recv.at[unit],
            at(0, 0, ways[way]),
        )

    def far_copy(unit):
        span = pl.ds(0, len(units[unit]) * rows + 8)
        return remote(
            one_out.at[unit, 0, span], one_in.at[unit, 0, span], one_send.at[unit], one_recv.at[unit], at(0, 0, 2)
        )

    def two_copy(unit, way):
        span = pl.ds(0, len(units[unit]) * rows + 8)
        return remote(
            two_out.at[unit, way, span], two_in.at[unit, way, span], two_send.at[unit], two_recv.at[unit],
            at(0, 0, ways[way]),
        )

    def project(first, count):
        numbers = [spot(*place) for place in shards_at[first:first + count]]
        right = jnp.concatenate([
            jnp.concatenate([down[core, f, q] for f in numbers], axis=1) for core in (0, 1) for q in range(QUARTERS)
        ], axis=0)
        parts = 1 if count > 2 else 2
        tall = 4 * rows // parts
        for part in range(parts):
            span = slice(part * tall, (part + 1) * tall)
            left = jnp.concatenate([hidden[slot, span] for slot in range(2 * QUARTERS)], axis=1)
            total = jnp.dot(left, right, preferred_element_type=jnp.float32)
            for n in range(count):
                shard = first + n
                acc[shard // 2, span, (shard % 2) * width:(shard % 2 + 1) * width] = total[:, n * width:(n + 1) * width]

    def pack(ref, unit, way, codes, level):
        tall = codes[0].shape[0]
        for n, code in enumerate(codes):
            ref[unit, way, n * tall:(n + 1) * tall] = code
        ref[unit, way, len(codes) * tall:len(codes) * tall + 8] = level

    def gather_terms(unit, first, last):
        return jnp.concatenate([terms(shard, first, last) for shard in units[unit]], axis=1)

    def launch(unit):
        if unit in direct:
            pack(one_out, unit, 0, *encode(gather_terms(unit, 3 * rows, 4 * rows)))
            far_copy(unit).start()
            for way in (0, 1):
                pack(two_out, unit, way, *encode(gather_terms(unit, (1 + way) * rows, (2 + way) * rows)))
                two_copy(unit, way).start()
        else:
            for way in (0, 1):
                first = 3 * rows + way * mid
                pack(one_out, unit, way, *encode(gather_terms(unit, first, first + mid)))
                one_copy(unit, way).start()

    def relay(unit):
        count = len(units[unit])
        ref = one_in.at[unit, :, pl.ds(0, count * mid + 8)]
        remote(ref, ref, one_send.at[unit], one_recv.at[unit], sibling).wait_recv()
        for way in (0, 1):
            level = level_of(one_in, unit, way, count * mid)
            sums = []
            for n, shard in enumerate(units[unit]):
                taken = decode(one_in[unit, way, n * mid:(n + 1) * mid], level)
                halves = [terms(shard, (1 + way) * rows + part * mid, (1 + way) * rows + (part + 1) * mid) for part in (0, 1)]
                halves[way] = halves[way] + taken
                sums.append(jnp.concatenate(halves, axis=0))
            pack(two_out, unit, way, *encode(jnp.concatenate(sums, axis=1)))
            two_copy(unit, way).start()

    def finish(unit):
        count = len(units[unit])
        ref = two_in.at[unit, :, pl.ds(0, count * rows + 8)]
        remote(ref, ref, two_send.at[unit], two_recv.at[unit], sibling).wait_recv()
        incoming = [(two_in, 0), (two_in, 1)]
        if unit in direct:
            far_copy(unit).wait_recv()
            incoming.append((one_in, 0))
        levels = [level_of(buf, unit, way, count * rows) for buf, way in incoming]
        for n, shard in enumerate(units[unit]):
            total = terms(shard, 0, rows)
            for (buf, way), level in zip(incoming, levels):
                total = total + decode(buf[unit, way, n * rows:(n + 1) * rows], level)
            f = spot(*shards_at[shard])
            out_ref[:, pl.ds(pl.multiple_of(f * width, width), width)] = total.astype(jnp.bfloat16)

    shards_at = [
        (0, 0), (-1, 0), (1, 0), (0, -1), (0, 1), (-1, -1), (-1, 1), (1, -1), (1, 1), (2, 0), (0, 2),
        (2, -1), (2, 1), (-1, 2), (1, 2), (2, 2),
    ]
    units = [(0,), (1, 2), (3, 4), (5, 6), (7, 8), (9, 10), (11, 12), (13, 14), (15,)]
    direct = (0, 1, 2, 5)

    downs.near(1)
    downs.wait_over(0)
    project(0, 1)
    launch(0)
    downs.own(0)
    downs.own(1)
    downs.far()
    downs.wait_over(1)
    downs.wait_over(2)
    project(1, 4)
    launch(1)
    launch(2)
    downs.wide(0)
    downs.wait_over(3)
    downs.wide(1)
    finish(0)
    downs.wait_over(5)
    project(5, 4)
    launch(3)
    launch(4)
    downs.back()
    downs.mid(0)
    downs.wait_over(4)
    project(9, 2)
    launch(5)
    downs.mid(1)
    downs.late(0)
    relay(3)
    downs.wait_over(6)
    project(11, 2)
    launch(6)
    relay(4)
    downs.late(1)
    finish(1)
    finish(2)
    downs.end()
    downs.wait_over(7)
    project(13, 2)
    launch(7)
    downs.wait_over(8)
    project(15, 1)
    launch(8)
    relay(6)
    relay(7)
    relay(8)
    finish(3)
    finish(4)
    finish(5)
    finish(6)
    finish(7)
    finish(8)

    ref = tok.at[pl.ds(0, 3)]
    remote(ref, ref, tok_send, tok_send, sibling).wait_send()
    for unit in range(len(units)):
        for way in (0, 1):
            two_copy(unit, way).wait_send()
            if unit not in direct:
                one_copy(unit, way).wait_send()
        if unit in direct:
            far_copy(unit).wait_send()
    ups.drain()
    downs.drain()


def solution(mesh):
    fs, tp = mesh.shape["fs"], mesh.shape["tp"]
    placed = (P(("fs", "tp"), None), P(), P("fs", "tp"), P("tp", "fs"))

    def whole(tokens, norm_gain, up_weight, down_weight):
        rows, depth = tokens.shape
        share, span = up_weight.shape
        width = down_weight.shape[1]
        piece = span // QUARTERS
        groups = tp // 2
        vm, dma = pltpu.VMEM, pltpu.SemaphoreType.DMA
        low, full = jnp.bfloat16, jnp.float32
        return pl.pallas_call(
            kernel,
            out_shape=jax.ShapeDtypeStruct((rows, depth), low),
            in_specs=[pl.BlockSpec(memory_space=pltpu.HBM)] * 4,
            out_specs=pl.BlockSpec(memory_space=pltpu.VMEM),
            scratch_shapes=[
                vm((rows, depth), low),
                vm((1, depth), full),
                vm((share, span), full),
                vm((span, width), full),
                vm((groups, rows, depth), low),
                vm((2, fs, QUARTERS, share, piece), low),
                vm((2, fs, QUARTERS, piece, width), low),
                vm((2 * QUARTERS, groups * rows, piece), full),
                vm((2 * QUARTERS, groups * rows, piece), low),
                vm((UNITS, 2, 2 * rows + 8, LANES), low),
                vm((UNITS, 2, 2 * rows + 8, LANES), low),
                vm((UNITS, 2, 2 * rows + 8, LANES), low),
                vm((UNITS, 2, 2 * rows + 8, LANES), low),
                dma((4,)), dma, dma((3,)),
                dma((2, 13)), dma((2, 9)), dma((2,)), dma((2,)), dma((UNITS,)), dma((UNITS,)), dma((UNITS,)), dma((UNITS,)),
            ],
            compiler_params=pltpu.CompilerParams(
                collective_id=0, has_side_effects=True, vmem_limit_bytes=VMEM_LIMIT
            ),
        )(*(
            pltpu.with_memory_space_constraint(array, pltpu.HBM)
            for array in (tokens, norm_gain.reshape(1, depth), up_weight, down_weight)
        ))

    return jax.shard_map(
        whole, mesh=mesh, in_specs=placed, out_specs=P(("fs", "tp"), None), check_vma=False
    )
```

```python
import functools

import jax
import jax.numpy as jnp
from jax import lax
from jax.experimental import pallas as pl
from jax.experimental.pallas import tpu as pltpu
from jax.sharding import PartitionSpec as P

epsilon = 1e-06
MESH = pl.DeviceIdType.MESH
VMEM_LIMIT = 48_000_000
SIDE = 4
QUARTERS = 4
LANES = 128
UNITS = 9
POWER = 9
PEAK = 11585.0
TINY = 1e-30


def encode(block):
    largest = jnp.max(jnp.abs(block), axis=0, keepdims=True)
    level = largest[:, :LANES]
    for start in range(LANES, block.shape[1], LANES):
        level = jnp.maximum(level, largest[:, start:start + LANES])
    level = jnp.maximum(level, TINY).astype(jnp.bfloat16)
    factor = PEAK / level.astype(jnp.float32)
    codes = []
    for start in range(0, block.shape[1], LANES):
        t = block[:, start:start + LANES] * factor
        t2 = t * t
        t4 = t2 * t2
        codes.append((t4 * t4 * t).astype(jnp.bfloat16))
    return codes, jnp.broadcast_to(level, (8, LANES))


def decode(code, level):
    y = code.astype(jnp.float32)
    size = jnp.exp(jnp.log(jnp.maximum(jnp.abs(y), 1e-38)) * (1.0 / POWER)) * (level * (1.0 / PEAK))
    return jnp.where(y > 0.0, size, jnp.where(y < 0.0, -size, 0.0))


def kernel(
    tok_hbm, gain_hbm, up_hbm, down_hbm, out_ref,
    tok_ref, gain_ref, up_ref, down_ref, tok, up, down, acc, hidden, one_out, one_in, two_out, two_in,
    load, tok_send, tok_recv, arrived, crossed, sent, side_sent, one_send, one_recv, two_send, two_recv,
):
    fs, tp = lax.axis_index("fs"), lax.axis_index("tp")
    z, y = fs // SIDE, lax.rem(fs, SIDE)
    x, c = tp // 2, lax.rem(tp, 2)
    other = 1 - c
    mine = fs
    rows = tok.shape[1]
    share = up.shape[3]
    piece = up.shape[4]
    width = down.shape[4]

    def ring(place, step):
        return lax.rem(place + (step + SIDE), SIDE)

    def at(dz, dy, dx):
        return (ring(z, dz) * SIDE + ring(y, dy), ring(x, dx) * 2 + c)

    sibling = (fs, x * 2 + other)

    def remote(src, dst, send, recv, to):
        return pltpu.make_async_remote_copy(
            src_ref=src, dst_ref=dst, send_sem=send, recv_sem=recv, device_id=to, device_id_type=MESH
        )

    barrier = pltpu.get_barrier_semaphore()
    peers = [at(1, 0, 0), at(-1, 0, 0), at(0, 1, 0), at(0, -1, 0), at(0, 0, 1), at(0, 0, -1), at(0, 0, 2), sibling]
    for to in peers:
        pl.semaphore_signal(barrier, inc=1, device_id=to, device_id_type=MESH)

    loads = [
        pltpu.make_async_copy(src, dst, load.at[n])
        for n, (src, dst) in enumerate([(up_hbm, up_ref), (tok_hbm, tok_ref), (gain_hbm, gain_ref), (down_hbm, down_ref)])
    ]
    for copy in loads:
        copy.start()

    def block(h, ia, ib):
        dz, dy = (ia, ib) if h == 0 else (ib, ia)
        return ring(z, dz) * SIDE + ring(y, dy)

    ways = (1, -1)
    NEAR, OWN, FAR, BACK, WIDE, MID, LATE, END = 0, 2, 4, 5, 6, 8, 10, 12

    class Gather:
        def __init__(self, number, buf, skew):
            self.number, self.buf, self.skew = number, buf, skew

        def send(self, h, ia, ib, j, axis, s, group):
            along_z = (axis == "a") == (h == 0)
            to = at(s, 0, 0) if along_z else at(0, s, 0)
            ref = self.buf.at[c, block(h, ia, ib), 2 * h + j]
            remote(ref, ref, sent.at[self.number], arrived.at[self.number, group], to).start()

        def wait(self, group, count=4):
            ref = self.buf.at[c, pl.ds(0, count), 0]
            remote(ref, ref, sent.at[self.number], arrived.at[self.number, group], sibling).wait_recv()

        def over(self, h, ia, ib, j, event):
            ref = self.buf.at[c, block(h, ia, ib), 2 * h + j]
            remote(ref, ref, side_sent.at[self.number], crossed.at[self.number, event], sibling).start()

        def wait_over(self, *events):
            for event in events:
                ref = self.buf.at[other, pl.ds(0, (2, 4, 4, 2, 2, 8, 4, 4, 2)[event]), pl.ds(0, 2)]
                remote(ref, ref, side_sent.at[self.number], crossed.at[self.number, event], sibling).wait_recv()

        def first(self):
            for axis, group in (("a", NEAR), ("b", OWN)):
                for turn in (0, 1):
                    for h in (0, 1):
                        for s in ways:
                            self.send(h, 0, 0, turn if s > 0 else 1 - turn, axis, s, group + turn)
            for h in (0, 1):
                for j in (0, 1):
                    self.over(h, 0, 0, j, 0)

        def out(self, turn):
            for h in (0, 1):
                for ia in (-1, 1):
                    for s in ways:
                        self.send(h, ia, 0, turn if ia < 0 else 1 - turn, "b", s, WIDE + turn)

        def near(self, turn):
            self.wait(NEAR + turn)
            if turn == 0:
                for h in (0, 1):
                    for s in ways:
                        self.send(h, -s, 0, 0 if s > 0 else 1, "a", s, FAR)
            self.out(turn)
            for h in (0, 1):
                for s in ways:
                    self.over(h, -s, 0, turn if s > 0 else 1 - turn, 1)

        def own(self, turn):
            self.wait(OWN + turn)
            if turn == 0:
                for h in (0, 1):
                    for s in ways:
                        self.send(h, 0, -s, 0 if s > 0 else 1, "b", s, BACK)
            for h in (0, 1):
                for s in ways:
                    self.over(h, 0, -s, turn if s > 0 else 1 - turn, 2)

        def out_far(self, h, turn):
            group = LATE + 1 if h == 1 and turn == 1 and self.skew else MID + turn
            for s in ways:
                self.send(h, 2, 0, turn if s > 0 else 1 - turn, "b", s, group)

        def far(self):
            self.wait(FAR)
            for turn in (0, 1):
                for h in (0, 1):
                    if h == 0 or turn == 0 or not self.skew:
                        self.out_far(h, turn)
            for h in (0, 1):
                for j in (0, 1):
                    self.over(h, 2, 0, j, 3)

        def back(self):
            self.wait(BACK)
            for h in (0, 1):
                for j in (0, 1):
                    self.over(h, 0, 2, j, 4)

        def wide(self, turn):
            self.wait(WIDE + turn, 8)
            for h in (0, 1):
                for s in ways:
                    ia = -s if turn == 0 else s
                    group = (MID + 1, LATE)[turn] if h == 1 and self.skew else LATE + turn
                    self.send(h, ia, -s, 0 if s > 0 else 1, "b", s, group)
            if turn == 1 and self.skew:
                self.out_far(1, 1)
            for h in (0, 1):
                for ia in (-1, 1):
                    for s in ways:
                        self.over(h, ia, -s, turn if ia < 0 else 1 - turn, 5)

        def crossed_far(self, h, turn, event):
            if turn == 0:
                for s in ways:
                    self.send(h, 2, -s, 0 if s > 0 else 1, "b", s, END)
            for s in ways:
                self.over(h, 2, -s, turn if s > 0 else 1 - turn, event)

        def crossed_edge(self, h, turn, event):
            for s in ways:
                self.over(h, -s if turn == 0 else s, 2, 0 if s > 0 else 1, event)

        def mid(self, turn):
            self.wait(MID + turn)
            self.crossed_far(0, turn, 6)
            if not self.skew:
                self.crossed_far(1, turn, 6)
            elif turn == 0:
                self.crossed_far(1, 0, 7)
            else:
                self.crossed_edge(1, 0, 6)

        def late(self, turn):
            self.wait(LATE + turn)
            self.crossed_edge(0, turn, 7)
            if not self.skew:
                self.crossed_edge(1, turn, 7)
            elif turn == 0:
                self.crossed_edge(1, 1, 6)
            else:
                self.crossed_far(1, 1, 7)

        def end(self):
            self.wait(END)
            for h in (0, 1):
                for j in (0, 1):
                    self.over(h, 2, 2, j, 8)

        def drain(self):
            ref = self.buf.at[0, pl.ds(0, self.buf.shape[1] - 1)]
            remote(ref, ref, sent.at[self.number], sent.at[self.number], sibling).wait_send()
            whole = self.buf.at[0]
            remote(whole, whole, side_sent.at[self.number], side_sent.at[self.number], sibling).wait_send()

    ups = Gather(0, up, False)
    downs = Gather(1, down, True)

    loads[0].wait()
    for q in range(QUARTERS):
        up[c, mine, q] = up_ref[:, q * piece:(q + 1) * piece].astype(jnp.bfloat16)
    pl.semaphore_wait(barrier, len(peers))
    ups.first()

    loads[1].wait()
    loads[2].wait()
    values = tok_ref[...].astype(jnp.float32)
    scale = lax.rsqrt(jnp.mean(values * values, axis=-1, keepdims=True) + epsilon)
    tok[x] = (values * scale * gain_ref[...]).astype(jnp.bfloat16)
    half = rows // 2

    def token_send(slot, part, s, group):
        ref = tok.at[slot, pl.ds(part * half, half)]
        remote(ref, ref, tok_send, tok_recv.at[group], at(0, 0, s)).start()

    def token_wait(group):
        ref = tok.at[0]
        remote(ref, ref, tok_send, tok_recv.at[group], sibling).wait_recv()

    for turn in (0, 1):
        for s in (1, -1):
            token_send(x, turn if s > 0 else 1 - turn, s, turn)
    loads[3].wait()
    for q in range(QUARTERS):
        down[c, mine, q] = down_ref[q * piece:(q + 1) * piece, :].astype(jnp.bfloat16)

    relative = (0, 1, -1, 2)

    def expand(places, begin, end, first_row, last_row):
        for h in (0, 1):
            numbers = [block(h, *place) for place in places]
            left = jnp.concatenate([
                jnp.concatenate(
                    [tok[ring(x, relative[r]), :, pl.ds(pl.multiple_of(f * share, share), share)] for f in numbers], axis=1
                ) for r in range(first_row, last_row)
            ], axis=0)
            span = slice(first_row * rows, last_row * rows)
            for core in (0, 1):
                slots = [core * QUARTERS + 2 * h + j for j in (0, 1)]
                right = jnp.concatenate([
                    jnp.concatenate([up[core, f, 2 * h + j] for f in numbers], axis=0) for j in (0, 1)
                ], axis=1)
                pre = jnp.dot(left, right, preferred_element_type=jnp.float32)
                for j, slot in enumerate(slots):
                    new = pre[:, j * piece:(j + 1) * piece]
                    if not begin:
                        new = new + acc[slot, span]
                    if end:
                        hidden[slot, span] = jnp.square(jnp.maximum(new, 0.0)).astype(jnp.bfloat16)
                    else:
                        acc[slot, span] = new

    groups = [
        [(0, 0), (-1, 0), (1, 0), (2, 0)], [(-1, -1), (-1, 1), (1, -1), (1, 1)], [(0, -1), (0, 1)],
        [(2, -1), (2, 1)], [(-1, 2), (1, 2)], [(0, 2), (2, 2)],
    ]

    ups.near(0)
    ups.near(1)
    ups.own(0)
    ups.own(1)
    ups.far()
    token_wait(0)
    for s in ways:
        token_send(ring(x, -s), 0 if s > 0 else 1, s, 2)
    ups.wide(0)
    token_wait(1)
    ups.wait_over(0, 1, 3)
    expand(groups[0], True, False, 0, 3)
    ups.wide(1)
    ups.back()
    ups.wait_over(5)
    expand(groups[1], False, False, 0, 3)
    ups.mid(0)
    ups.wait_over(2)
    expand(groups[2], False, False, 0, 3)
    ups.mid(1)
    downs.first()
    token_wait(2)
    expand(groups[0], True, False, 3, 4)
    expand(groups[1], False, False, 3, 4)
    expand(groups[2], False, False, 3, 4)
    ups.late(0)
    ups.late(1)
    ups.wait_over(6)
    expand(groups[3], False, False, 0, 4)
    ups.end()
    ups.wait_over(7)
    expand(groups[4], False, False, 0, 4)
    downs.near(0)
    ups.wait_over(4, 8)
    expand(groups[5], False, True, 0, 4)

    def spot(dz, dy):
        return ring(z, dz) * SIDE + ring(y, dy)

    def level_of(ref, unit, way, at_row):
        return ref[unit, way, at_row:at_row + 8].astype(jnp.float32)[0:1]

    def terms(shard, first, last):
        return acc[shard // 2, first:last, (shard % 2) * width:(shard % 2 + 1) * width]

    mid = rows // 2

    def one_copy(unit, way):
        span = pl.ds(0, len(units[unit]) * mid + 8)
        return remote(
            one_out.at[unit, way, span], one_in.at[unit, way, span], one_send.at[unit], one_recv.at[unit],
            at(0, 0, ways[way]),
        )

    def far_copy(unit):
        span = pl.ds(0, len(units[unit]) * rows + 8)
        return remote(
            one_out.at[unit, 0, span], one_in.at[unit, 0, span], one_send.at[unit], one_recv.at[unit], at(0, 0, 2)
        )

    def two_copy(unit, way):
        span = pl.ds(0, len(units[unit]) * rows + 8)
        return remote(
            two_out.at[unit, way, span], two_in.at[unit, way, span], two_send, two_recv.at[unit],
            at(0, 0, ways[way]),
        )

    def project(first, count):
        numbers = [spot(*place) for place in shards_at[first:first + count]]
        right = jnp.concatenate([
            jnp.concatenate([down[core, f, q] for f in numbers], axis=1) for core in (0, 1) for q in range(QUARTERS)
        ], axis=0)
        parts = 1 if count > 2 else 2
        tall = 4 * rows // parts
        for part in range(parts):
            span = slice(part * tall, (part + 1) * tall)
            left = jnp.concatenate([hidden[slot, span] for slot in range(2 * QUARTERS)], axis=1)
            total = jnp.dot(left, right, preferred_element_type=jnp.float32)
            for n in range(count):
                shard = first + n
                acc[shard // 2, span, (shard % 2) * width:(shard % 2 + 1) * width] = total[:, n * width:(n + 1) * width]

    def pack(ref, unit, way, codes, level):
        tall = codes[0].shape[0]
        for n, code in enumerate(codes):
            ref[unit, way, n * tall:(n + 1) * tall] = code
        ref[unit, way, len(codes) * tall:len(codes) * tall + 8] = level

    def gather_terms(unit, first, last):
        return jnp.concatenate([terms(shard, first, last) for shard in units[unit]], axis=1)

    def launch(unit):
        if unit in direct:
            pack(one_out, unit, 0, *encode(gather_terms(unit, 3 * rows, 4 * rows)))
            far_copy(unit).start()
            for way in (0, 1):
                pack(two_out, unit, way, *encode(gather_terms(unit, (1 + way) * rows, (2 + way) * rows)))
                two_copy(unit, way).start()
        else:
            for way in (0, 1):
                first = 3 * rows + way * mid
                pack(one_out, unit, way, *encode(gather_terms(unit, first, first + mid)))
                one_copy(unit, way).start()

    def relay(unit):
        count = len(units[unit])
        ref = one_in.at[unit, :, pl.ds(0, count * mid + 8)]
        remote(ref, ref, one_send.at[unit], one_recv.at[unit], sibling).wait_recv()
        for way in (0, 1):
            level = level_of(one_in, unit, way, count * mid)
            sums = []
            for n, shard in enumerate(units[unit]):
                taken = decode(one_in[unit, way, n * mid:(n + 1) * mid], level)
                halves = [terms(shard, (1 + way) * rows + part * mid, (1 + way) * rows + (part + 1) * mid) for part in (0, 1)]
                halves[way] = halves[way] + taken
                sums.append(jnp.concatenate(halves, axis=0))
            pack(two_out, unit, way, *encode(jnp.concatenate(sums, axis=1)))
            two_copy(unit, way).start()

    def finish(unit):
        count = len(units[unit])
        ref = two_in.at[unit, :, pl.ds(0, count * rows + 8)]
        remote(ref, ref, two_send, two_recv.at[unit], sibling).wait_recv()
        incoming = [(two_in, 0), (two_in, 1)]
        if unit in direct:
            far_copy(unit).wait_recv()
            incoming.append((one_in, 0))
        levels = [level_of(buf, unit, way, count * rows) for buf, way in incoming]
        for n, shard in enumerate(units[unit]):
            total = terms(shard, 0, rows)
            for (buf, way), level in zip(incoming, levels):
                total = total + decode(buf[unit, way, n * rows:(n + 1) * rows], level)
            f = spot(*shards_at[shard])
            out_ref[:, pl.ds(pl.multiple_of(f * width, width), width)] = total.astype(jnp.bfloat16)

    shards_at = [
        (0, 0), (-1, 0), (1, 0), (0, -1), (0, 1), (-1, -1), (-1, 1), (1, -1), (1, 1), (2, 0), (0, 2),
        (2, -1), (2, 1), (-1, 2), (1, 2), (2, 2),
    ]
    units = [(0,), (1, 2), (3, 4), (5, 6), (7, 8), (9, 10), (11, 12), (13, 14), (15,)]
    direct = (0, 1, 2)

    downs.near(1)
    downs.wait_over(0)
    project(0, 1)
    launch(0)
    downs.own(0)
    downs.own(1)
    downs.far()
    downs.wait_over(1)
    downs.wait_over(2)
    project(1, 4)
    launch(1)
    launch(2)
    downs.wide(0)
    downs.wait_over(3)
    downs.wide(1)
    finish(0)
    downs.wait_over(5)
    project(5, 4)
    launch(3)
    launch(4)
    downs.back()
    downs.mid(0)
    downs.wait_over(4)
    project(9, 2)
    launch(5)
    downs.mid(1)
    downs.late(0)
    relay(3)
    downs.wait_over(6)
    project(11, 2)
    launch(6)
    relay(4)
    downs.late(1)
    finish(1)
    finish(2)
    downs.end()
    downs.wait_over(7)
    project(13, 2)
    launch(7)
    downs.wait_over(8)
    project(15, 1)
    launch(8)
    relay(5)
    relay(6)
    relay(7)
    relay(8)
    finish(3)
    finish(4)
    finish(5)
    finish(6)
    finish(7)
    finish(8)

    ref = tok.at[pl.ds(0, 3)]
    remote(ref, ref, tok_send, tok_send, sibling).wait_send()
    for unit in range(len(units)):
        for way in (0, 1):
            if unit not in direct:
                one_copy(unit, way).wait_send()
        if unit in direct:
            far_copy(unit).wait_send()
    ref = hidden.at[pl.ds(0, 5), pl.ds(0, 424)]
    remote(ref, ref, two_send, two_send, sibling).wait_send()
    ups.drain()
    downs.drain()


def solution(mesh):
    fs, tp = mesh.shape["fs"], mesh.shape["tp"]
    placed = (P(("fs", "tp"), None), P(), P("fs", "tp"), P("tp", "fs"))

    def whole(tokens, norm_gain, up_weight, down_weight):
        rows, depth = tokens.shape
        share, span = up_weight.shape
        width = down_weight.shape[1]
        piece = span // QUARTERS
        groups = tp // 2
        vm, dma = pltpu.VMEM, pltpu.SemaphoreType.DMA
        low, full = jnp.bfloat16, jnp.float32
        return pl.pallas_call(
            kernel,
            out_shape=jax.ShapeDtypeStruct((rows, depth), low),
            in_specs=[pl.BlockSpec(memory_space=pltpu.HBM)] * 4,
            out_specs=pl.BlockSpec(memory_space=pltpu.VMEM),
            scratch_shapes=[
                vm((rows, depth), low),
                vm((1, depth), full),
                vm((share, span), full),
                vm((span, width), full),
                vm((groups, rows, depth), low),
                vm((2, fs, QUARTERS, share, piece), low),
                vm((2, fs, QUARTERS, piece, width), low),
                vm((2 * QUARTERS, groups * rows, piece), full),
                vm((2 * QUARTERS, groups * rows, piece), low),
                vm((UNITS, 2, 2 * rows + 8, LANES), low),
                vm((UNITS, 2, 2 * rows + 8, LANES), low),
                vm((UNITS, 2, 2 * rows + 8, LANES), low),
                vm((UNITS, 2, 2 * rows + 8, LANES), low),
                dma((4,)), dma, dma((3,)),
                dma((2, 13)), dma((2, 9)), dma((2,)), dma((2,)), dma((UNITS,)), dma((UNITS,)), dma, dma((UNITS,)),
            ],
            compiler_params=pltpu.CompilerParams(
                collective_id=0, has_side_effects=True, vmem_limit_bytes=VMEM_LIMIT
            ),
        )(*(
            pltpu.with_memory_space_constraint(array, pltpu.HBM)
            for array in (tokens, norm_gain.reshape(1, depth), up_weight, down_weight)
        ))

    return jax.shard_map(
        whole, mesh=mesh, in_specs=placed, out_specs=P(("fs", "tp"), None), check_vma=False
    )
```
